32 devices in a mesh: ep: 8 (over z, x), tp: 4 (over y, core).
Axes of the slice: x: 2, y: 2, z: 4, core: 2. Of those that a mesh axis runs over, the one named last changes fastest.
Arguments:
- q_in: bfloat16 [4096, 1024], P('ep', 'tp'), may hold values from -6 to 6
- k_in: bfloat16 [4096, 256], P('ep'), may hold values from -6 to 6
- v_in: bfloat16 [4096, 256], P('ep'), may hold values from -6 to 6
- q_gain: float32 [64], replicated, may hold values from 0.1 to 1.9
- k_gain: float32 [64], replicated, may hold values from 0.1 to 1.9
- w_out: bfloat16 [1024, 2048], P('tp'), may hold values from -0.1875 to 0.1875
- post_gain: float32 [2048], replicated, may hold values from 0.1 to 1.9
- moe_in: bfloat16 [1024, 2048], P('ep'), may hold values from -6 to 6
- routes: int32 [1024, 2], P('ep'), may hold values from 0 to 7, all different within a row; in each aligned block of 128 rows (0 to 127, 128 to 255, ...) at most 48 rows name the same one
- route_logits: float32 [1024, 2], P('ep'), may hold values from -6 to 6
- pre_gain: float32 [2048], replicated, may hold values from 0.1 to 1.9
- w_gate: bfloat16 [8, 2048, 4096], P('ep', None, 'tp'), may hold values from -0.125 to 0.125
- w_up: bfloat16 [8, 2048, 4096], P('ep', None, 'tp'), may hold values from -0.125 to 0.125
- w_down: bfloat16 [8, 4096, 2048], P('ep', 'tp'), may hold values from -0.125 to 0.125
Outputs:
- attn_out: bfloat16 [4096, 2048], P(('ep', 'tp'))
- moe_out: bfloat16 [1024, 2048], P('ep', 'tp')
The draws below stay inside these ranges and needn't reach their ends.
Inputs may be any that keep to these rules, and one draw needn't show every extreme that they name: `routes`: each row names 2 different experts. Among the rows of one index of ep no expert is named by more than 48 rows, a bound that some block reaches of them.
All inputs are finite; a program needn't handle non-finite values.
Results may differ from the reference program's by a relative error of at most 0.018.
Values may be sent and summed in bfloat16 or wider, within the bound.
A program may use at most 64 MiB of HBM per device.

```python
import math
import jax
import jax.numpy as jnp
import numpy as np
from jax import lax

D = 2048
HEADS = 16
KV_HEADS = 4
HEAD = 64
GRID_W = 128
FFE = 4096
TOP = 2
TOKM_DEV = 128
SEQ = 4096
TOKM = 1024
EXPERTS = 8
HEADS_DEV = 4
FF_DEV = 1024
CAP = 48
N_EP = 8
N_TP = 4


def strengthened(drawn, own_key, source, target, shards_of, factor):
    def block_of(axis_at):
        return (jnp.arange(drawn.shape[axis_at]) // (drawn.shape[axis_at] // shards_of)).reshape((-1,) + (1,) * (drawn.ndim - 1 - axis_at))

    one_side = jax.random.permutation(own_key, shards_of)[block_of(target)]
    far = (block_of(target) + shards_of // 2) % shards_of
    return jnp.where((block_of(source) == one_side) | (block_of(source) == far), factor * drawn, drawn)


def block_levels(key, extent, shards, low, largest):
    factor_of, own = 1.0, jax.random.fold_in(key, 6)
    for dim, shards_of in shards:
        heights = jnp.exp(jax.random.uniform(jax.random.fold_in(own, dim), (shards_of,), jnp.float32, low / len(shards), largest / len(shards)))
        factor_of = factor_of * jnp.repeat(heights, extent[dim] // shards_of).reshape([-1 if axis == dim else 1 for axis in range(len(extent))])
    return factor_of


def assign_block(own_key, own, number, rows, number_of, top, bound, slope):
    order = jax.random.permutation(own_key, number_of)
    heavy_load, usual = load_shares(number_of, rows * top, bound, slope, True), load_shares(number_of, rows * top, bound, slope, False)
    places = jnp.arange(number_of)

    def named(lengths, offset_by):
        used = int((lengths > 0).sum())
        fixed = max(1, used // 4)
        shifted = fixed + (places - fixed + offset_by * (used - fixed)) % max(1, number_of - fixed)
        return jnp.zeros((number_of,), jnp.int32).at[order[jnp.where(places < fixed, places, shifted)]].set(jnp.asarray(lengths, jnp.int32))

    lengths = jnp.where(number % 4 == 0, named(heavy_load, number // 4), named(usual, number - number // 4 - 1))
    mixed = jax.random.permutation(jax.random.fold_in(own, 3), number_of)
    source_of, taker = mixed[0:number_of // 2 * 2:2], mixed[1:number_of // 2 * 2:2]
    margin = jnp.minimum(lengths[source_of] - 1, bound - lengths[taker]) // 2
    margin = jnp.where((source_of == order[0]) | (taker == order[0]) | (lengths[taker] == 0), 0, jnp.maximum(margin, 0))
    shifted = jax.random.randint(jax.random.fold_in(own, 4), (number_of // 2,), 0, 1 << 20) % (margin + 1)
    lengths = lengths.at[source_of].add(-shifted).at[taker].add(shifted)
    labels = jnp.searchsorted(jnp.cumsum(lengths), jnp.arange(rows * top), side="right").astype(jnp.int32)
    grid = labels.reshape(top, rows).T
    grid = grid[jax.random.permutation(jax.random.fold_in(own, 1), rows)]
    offset_by = jax.random.randint(jax.random.fold_in(own, 2), (rows, 1), 0, top)
    return jnp.take_along_axis(grid, (jnp.arange(top)[None, :] + offset_by) % top, axis=1)


def load_shares(number_of, total, limit, slope, full):
    weights = [(1 << 20) // math.isqrt(rank ** slope) + 1 for rank in range(1, number_of + 1)]
    largest = limit if full else min(limit, max(-(-total // number_of), total * weights[0] // sum(weights)))
    least = 1 if total - largest >= number_of - 1 else 0
    given, surplus = [largest] + [least] * (number_of - 1), total - largest - least * (number_of - 1)
    while surplus > 0:
        movable = [i for i in range(1, number_of) if given[i] < largest] or [i for i in range(1, number_of) if given[i] < limit]
        pool, budget = sum([weights[i] for i in movable]), surplus
        for i in movable:
            extra = min(limit - given[i], max(1, budget * weights[i] // pool), surplus)
            given[i] = given[i] + extra
            surplus = surplus - extra
    return np.array(given)


def noise(stream_key, extent, deviation, reach, cuts=(), kind=jnp.bfloat16):
    drawn = deviation * jax.random.normal(stream_key, extent, jnp.float32)
    if cuts:
        drawn = drawn * block_levels(stream_key, extent, cuts, -0.22, 0.18)
    return jnp.clip(drawn, -reach, reach).astype(kind)


def heavy_noise(own_key, dims, deviation, most, pieces, heavy, held_as=jnp.bfloat16):
    result = deviation * jax.random.normal(own_key, dims, jnp.float32)
    if pieces:
        result = result * block_levels(own_key, dims, pieces, -0.22, 0.18)
    return jnp.clip(strengthened(result, jax.random.fold_in(own_key, 3), *heavy), -most, most).astype(held_as)


def setup_inputs(seed: int = 0) -> dict:
    arg_keys = jax.random.split(jax.random.key(seed), 15)
    q_in = noise(arg_keys[0], (SEQ, HEADS * HEAD), 1.0, 6.0, ((0, 8), (1, 4)))
    k_in = noise(arg_keys[1], (SEQ, KV_HEADS * HEAD), 1.0, 6.0, ((0, 8),))
    v_in = noise(arg_keys[2], (SEQ, KV_HEADS * HEAD), 1.0, 6.0, ((0, 8),))
    q_gain = jnp.clip(1.0 + 0.18 * jax.random.normal(arg_keys[3], (HEAD,), jnp.float32), 0.1, 1.9)
    k_gain = jnp.clip(1.0 + 0.18 * jax.random.normal(arg_keys[4], (HEAD,), jnp.float32), 0.1, 1.9)
    w_out = noise(arg_keys[5], (HEADS * HEAD, D), (HEADS * HEAD) ** -0.5, 0.1875, ((0, 4),))
    post_gain = jnp.clip(1.0 + 0.18 * jax.random.normal(arg_keys[6], (D,), jnp.float32), 0.1, 1.9)
    moe_in = noise(arg_keys[7], (TOKM, D), 1.0, 6.0, ((0, 8),))
    routes_keys = jax.random.split(jax.random.fold_in(arg_keys[8], 1), TOKM // TOKM_DEV)
    routes_turns = jax.random.permutation(jax.random.fold_in(arg_keys[8], 3), TOKM // TOKM_DEV)
    routes = jax.vmap(lambda own, number: assign_block(jax.random.fold_in(arg_keys[8], 2), own, number, TOKM_DEV, EXPERTS, TOP, CAP, 2))(routes_keys, routes_turns).reshape((TOKM, TOP))
    route_logits = noise(arg_keys[9], (TOKM, TOP), 1.5, 6.0, ((0, 8),), jnp.float32)
    pre_gain = jnp.clip(1.0 + 0.18 * jax.random.normal(arg_keys[10], (D,), jnp.float32), 0.1, 1.9)
    w_gate = noise(arg_keys[11], (EXPERTS, D, FFE), D ** -0.5, 0.125, ((0, 8), (2, 4)))
    w_up = noise(arg_keys[12], (EXPERTS, D, FFE), D ** -0.5, 0.125, ((0, 8), (2, 4)))
    w_down = heavy_noise(arg_keys[13], (EXPERTS, FFE, D), FFE ** -0.5, 0.125, ((0, 8), (1, 4)), (1, 2, 4, 2.0))
    return {"q_in": q_in, "k_in": k_in, "v_in": v_in, "q_gain": q_gain, "k_gain": k_gain, "w_out": w_out, "post_gain": post_gain, "moe_in": moe_in, "routes": routes, "route_logits": route_logits, "pre_gain": pre_gain, "w_gate": w_gate, "w_up": w_up, "w_down": w_down}


EPSILON = 1e-06
ROPE_BASE = 10000.0

def head_norm(values, gain):
    return values * lax.rsqrt(lax.optimization_barrier(jnp.mean(values * values, axis=-1, keepdims=True)) + EPSILON) * gain

def rotate_half(values, angles):
    quarter = angles.shape[-1]
    first_part = values[..., :quarter]
    second_part = values[..., quarter:]
    cosine = jnp.cos(angles)[:, None, :]
    sine_part = jnp.sin(angles)[:, None, :]
    return jnp.concatenate([first_part * cosine - second_part * sine_part, second_part * cosine + first_part * sine_part], axis=-1)

def grid_rotary(values, offset):
    row_count = values.shape[0]
    head_width = values.shape[-1]
    quarter = head_width // 4
    half_width = head_width // 2
    position = offset + jnp.arange(row_count, dtype=jnp.int32)
    grid_row = (position // GRID_W).astype(jnp.float32)
    grid_col = (position % GRID_W).astype(jnp.float32)
    inverse = ROPE_BASE ** (-jnp.arange(quarter, dtype=jnp.float32) / quarter)
    return jnp.concatenate([rotate_half(values[..., :half_width], grid_row[:, None] * inverse[None, :]), rotate_half(values[..., half_width:], grid_col[:, None] * inverse[None, :])], axis=-1)

def slot_table(route_rows, expert_count, capacity):
    token_count, top_count = route_rows.shape
    flat_routes = route_rows.reshape(-1).astype(jnp.int32)
    one_hot = (flat_routes[:, None] == jnp.arange(expert_count, dtype=jnp.int32)[None, :]).astype(jnp.int32)
    ranked = lax.optimization_barrier(jnp.sum((jnp.cumsum(one_hot, axis=0) - 1) * one_hot, axis=1))
    placed = (flat_routes * capacity + ranked).astype(jnp.int32)
    slot_owner = jnp.full((expert_count * capacity,), token_count * top_count, dtype=jnp.int32)
    slot_owner = slot_owner.at[placed].set(jnp.arange(token_count * top_count, dtype=jnp.int32))
    return (slot_owner, placed)

def mixer_half(q_in, k_in, v_in, q_gain, k_gain, w_out, post_gain):
    queries = head_norm(q_in.astype(jnp.float32).reshape(SEQ, HEADS, HEAD), q_gain.astype(jnp.float32))
    queries = grid_rotary(queries, 0).astype(jnp.bfloat16)
    keys = head_norm(k_in.astype(jnp.float32).reshape(SEQ, KV_HEADS, HEAD), k_gain.astype(jnp.float32))
    keys = grid_rotary(keys, 0).astype(jnp.bfloat16)
    repeat = HEADS // KV_HEADS
    key_float = keys.astype(jnp.float32)
    value_float = v_in.astype(jnp.float32).reshape(SEQ, KV_HEADS, HEAD)
    blocked = queries.reshape(SEQ // 128, 128, KV_HEADS, repeat, HEAD)

    def attend(query_block):
        scores = jnp.einsum('qgrd,kgd->grqk', query_block.astype(jnp.float32), key_float) * HEAD ** (-0.5)
        weights = jnp.exp(scores)
        denominator = lax.optimization_barrier(jnp.sum(weights, axis=-1))
        rounded = lax.optimization_barrier(weights.astype(jnp.bfloat16)).astype(jnp.float32)
        summed = jnp.einsum('grqk,kgd->qgrd', rounded, value_float)
        return (summed / jnp.transpose(denominator, (2, 0, 1))[..., None]).astype(jnp.bfloat16)
    head_out = lax.map(attend, blocked).reshape(SEQ, HEADS * HEAD)
    grouped_out = head_out.reshape(SEQ, N_TP, HEADS_DEV * HEAD)
    grouped_w = w_out.reshape(N_TP, HEADS_DEV * HEAD, D)

    def add_group(running, index):
        term = jnp.dot(grouped_out[:, index], grouped_w[index], preferred_element_type=jnp.float32)
        term = lax.optimization_barrier(term.astype(jnp.bfloat16))
        return (running + term.astype(jnp.float32), None)
    mixed, unused = lax.scan(add_group, jnp.zeros((SEQ, D), jnp.float32), jnp.arange(N_TP, dtype=jnp.int32))
    return head_norm(mixed, post_gain.astype(jnp.float32)).astype(jnp.bfloat16)

def experts_half(moe_in, routes, route_logits, pre_gain, w_gate, w_up, w_down):
    normed = head_norm(moe_in.astype(jnp.float32), pre_gain.astype(jnp.float32)).astype(jnp.bfloat16)
    copy_count = TOKM * TOP
    local_copies = TOKM_DEV * TOP
    padded = jnp.concatenate([normed, jnp.zeros((1, D), normed.dtype)], axis=0)
    blocks = routes.reshape(N_EP, TOKM_DEV, TOP)
    owners, unused = jax.vmap(lambda block_routes: slot_table(block_routes, EXPERTS, CAP))(blocks)
    shift_by = (jnp.arange(N_EP, dtype=jnp.int32) * local_copies)[:, None]
    global_owner = jnp.where(owners < local_copies, owners + shift_by, copy_count).astype(jnp.int32)
    per_expert = global_owner.reshape(N_EP, EXPERTS, CAP).transpose(1, 0, 2).reshape(EXPERTS, N_EP * CAP)

    def one_expert(results, inputs):
        owner_ids, gate_w, up_w, down_w = inputs
        gathered = padded[owner_ids // TOP]
        gate_pre = jnp.dot(gathered, gate_w, preferred_element_type=jnp.float32)
        up_pre = jnp.dot(gathered, up_w, preferred_element_type=jnp.float32)
        hidden = (jax.nn.silu(gate_pre) * up_pre).astype(jnp.bfloat16)
        hidden_groups = hidden.reshape(N_EP * CAP, N_TP, FF_DEV)
        down_groups = down_w.reshape(N_TP, FF_DEV, D)

        def add_group(running, index):
            term = jnp.dot(hidden_groups[:, index], down_groups[index], preferred_element_type=jnp.float32)
            term = lax.optimization_barrier(term.astype(jnp.bfloat16))
            return (running + term.astype(jnp.float32), None)
        combined, unused_out = lax.scan(add_group, jnp.zeros((N_EP * CAP, D), jnp.float32), jnp.arange(N_TP, dtype=jnp.int32))
        return (results.at[owner_ids].set(combined.astype(results.dtype)), None)
    results, unused_all = lax.scan(one_expert, jnp.zeros((copy_count + 1, D), jnp.bfloat16), (per_expert, w_gate, w_up, w_down))
    copies = results[:copy_count].reshape(TOKM, TOP, D).astype(jnp.float32)
    route_weight = jax.nn.softmax(route_logits.astype(jnp.float32), axis=-1)
    return lax.optimization_barrier(jnp.sum(route_weight[..., None] * copies, axis=1)).astype(jnp.bfloat16)

def reference(q_in, k_in, v_in, q_gain, k_gain, w_out, post_gain, moe_in, routes, route_logits, pre_gain, w_gate, w_up, w_down):
    attn_out = mixer_half(q_in, k_in, v_in, q_gain, k_gain, w_out, post_gain)
    moe_out = experts_half(moe_in, routes, route_logits, pre_gain, w_gate, w_up, w_down)
    return (attn_out, moe_out)
```

```python
import functools

import jax
import jax.numpy as jnp
import numpy as np
from jax import lax
from jax.experimental import pallas as pl
from jax.experimental.pallas import tpu as pltpu
from jax.sharding import PartitionSpec as P

GRID_W = 128
EPSILON = 1e-06
ROPE_BASE = 10000.0
MESH = pl.DeviceIdType.MESH


def turn_tables(positions, rows_of_grid, quarter):
    inverse = ROPE_BASE ** (-np.arange(quarter, dtype=np.float32) / np.float32(quarter))
    inverse = inverse.astype(np.float32)

    def table(count, first_half):
        angles = (np.arange(count, dtype=np.float32)[:, None] * inverse[None, :]).astype(np.float64)
        cos, sin = np.cos(angles), np.sin(angles)
        none = np.zeros_like(cos)
        cos = np.concatenate([cos, cos, none, none] if first_half else [none, none, cos, cos], axis=1)
        sin = np.concatenate([-sin, sin, none, none] if first_half else [none, none, -sin, sin], axis=1)
        return np.concatenate([cos, cos], axis=1), np.concatenate([sin, sin], axis=1)

    grid_rows = positions // rows_of_grid
    by_row = table(grid_rows, True)
    by_col = table(rows_of_grid, False)
    return [jnp.asarray(part, jnp.float32) for part in by_row + by_col]


def kernel(
    dims,
    route_ref, logit_ref, pre_ref, gain_ref, qg_ref, kg_ref, crow_ref, srow_ref, ccol_ref, scol_ref,
    q_hbm, k_hbm, v_hbm, x_hbm, wout_hbm, wg_hbm, wu_hbm, wd_hbm,
    attn_ref, moe_ref,
    q_in, k_in, v_in, x_ref, wout_ref, q_ref, pair_ref, placed_ref,
    outgo_ref, mixw_ref, wg, wu, wd, kvbuf, vx, kt, acc, arrived, hidden,
    pa, pa_in, pa_red, pa_in2, pm, pm_in, pm_red, pm_in2, summed, ret,
    in_sem, w_sem, loc_sem, kv_s, kv_r, disp_s, disp_r, rel_s, rel_r, fwd_s,
    a1_s, a1_r, a2_s, a2_r, m1_s, m1_r, m2_s, m2_r, ret_s, ret_r,
):
    n_ep, n_tp, heads, cap, repeat = dims
    ny = n_tp // 2
    ep = lax.axis_index("ep")
    tp = lax.axis_index("tp")
    core = lax.rem(tp, 2)
    row = tp // 2
    partner = row * 2 + 1 - core
    rows_kv = pair_ref.shape[0]
    dq = outgo_ref.shape[1]
    slots = outgo_ref.shape[0]
    piece = attn_ref.shape[0]

    def remote(src, dst, ss, rs, e, t):
        return pltpu.make_async_remote_copy(
            src_ref=src, dst_ref=dst, send_sem=ss, recv_sem=rs,
            device_id=(e, t), device_id_type=MESH,
        )

    def ep_at(d):
        return lax.rem(ep + d, n_ep)

    def ep_from(d):
        return lax.rem(ep - d + n_ep, n_ep)

    def same_core(d):
        return lax.rem(row + d, ny) * 2 + core

    def row_from(d):
        return lax.rem(row - d + ny, ny)

    def slot_rows(e):
        return pl.ds(pl.multiple_of(e * cap, cap), cap)

    head = qg_ref.shape[1]
    lane_count = 2 * head
    kv_index = tp * heads // repeat
    kv_lanes = pl.ds(pl.multiple_of((kv_index // 2) * lane_count, lane_count), lane_count)
    ins = [
        pltpu.make_async_copy(src, dst, in_sem.at[i])
        for i, (src, dst) in enumerate((
            (x_hbm, x_ref), (k_hbm.at[:, kv_lanes], k_in), (v_hbm.at[:, kv_lanes], v_in),
            (q_hbm, q_in), (wout_hbm, wout_ref),
        ))
    ]
    for copy in ins[:4]:
        copy.start()
    loads = [
        pltpu.make_async_copy(src, dst, w_sem.at[i])
        for i, (src, dst) in enumerate(((wg_hbm, wg), (wu_hbm, wu), (wd_hbm, wd)))
    ]
    barrier = pltpu.get_barrier_semaphore()
    for d in range(1, n_ep):
        pl.semaphore_signal(barrier, inc=1, device_id=(ep_at(d), tp), device_id_type=MESH)
    for d in range(1, ny):
        pl.semaphore_signal(barrier, inc=1, device_id=(ep, same_core(d)), device_id_type=MESH)
    pl.semaphore_signal(barrier, inc=1, device_id=(ep, partner), device_id_type=MESH)

    bf16, f32 = jnp.bfloat16, jnp.float32
    top, tokens = logit_ref.shape
    logits = logit_ref[...]
    power = jnp.exp(logits - jnp.max(logits, axis=0, keepdims=True))
    chance = power / jnp.sum(power, axis=0, keepdims=True)
    expert = lax.broadcasted_iota(jnp.int32, (n_ep, tokens), 0)
    named = jnp.zeros((n_ep, tokens), f32)
    share = jnp.zeros((n_ep, tokens), f32)
    for j in range(top):
        hit = route_ref[j : j + 1, :] == expert
        named = jnp.where(hit, 1.0, named)
        share = jnp.where(hit, chance[j : j + 1, :], share)
    above = lax.broadcasted_iota(jnp.int32, (tokens, tokens), 0) < lax.broadcasted_iota(
        jnp.int32, (tokens, tokens), 1
    )
    rank = jnp.dot(named, jnp.where(above, 1.0, 0.0), preferred_element_type=f32)
    rank = jnp.where(named > 0.0, rank, -1.0)
    place = lax.broadcasted_iota(jnp.int32, (cap, tokens), 0).astype(f32)
    for e in range(n_ep):
        there = rank[e : e + 1, :] == place
        placed_ref[e * cap : (e + 1) * cap, :] = jnp.where(there, 1.0, 0.0).astype(bf16)
        mixw_ref[e * cap : (e + 1) * cap, :] = jnp.where(there, share[e : e + 1, :], 0.0)

    ins[0].wait()
    x = x_ref[...].astype(f32)
    scale = lax.rsqrt(jnp.mean(x * x, axis=-1, keepdims=True) + EPSILON)
    mine = pl.ds(pl.multiple_of(tp * dq, dq), dq)
    normed = (x_ref[:, mine].astype(f32) * scale * pre_ref[:, mine]).astype(bf16)
    outgo_ref[...] = jnp.dot(placed_ref[...], normed, preferred_element_type=f32).astype(bf16)

    lane = lax.broadcasted_iota(jnp.int32, (GRID_W, lane_count), 1)
    first = lane < head
    ahead = lax.rem(lane, head // 2) < head // 4
    joined = lax.broadcasted_iota(jnp.int32, (lane_count, lane_count), 0) // head == (
        lax.broadcasted_iota(jnp.int32, (lane_count, lane_count), 1) // head
    )
    joined = jnp.where(joined, 1.0, 0.0).astype(bf16)
    blocks = rows_kv // GRID_W

    def turned(values, gain, b):
        square = values * values
        high = square.astype(bf16)
        low = (square - high.astype(f32)).astype(bf16)
        total = jnp.dot(high, joined, preferred_element_type=f32) + jnp.dot(
            low, joined, preferred_element_type=f32
        )
        values = values * lax.rsqrt(total * (1.0 / head) + EPSILON) * gain
        other = jnp.where(
            ahead,
            pltpu.roll(values, lane_count - head // 4, 1),
            pltpu.roll(values, head // 4, 1),
        )
        at = pl.ds(ep * blocks + b, 1)
        return values * (crow_ref[at, :] + ccol_ref[...]) + other * (srow_ref[at, :] + scol_ref[...])

    k_gain = jnp.concatenate([kg_ref[...], kg_ref[...]], axis=1)
    q_gain = jnp.concatenate([qg_ref[...], qg_ref[...]], axis=1)
    odd = lax.rem(kv_index, 2)
    ins[1].wait()
    ins[2].wait()
    for b in range(blocks):
        at = slice(b * GRID_W, (b + 1) * GRID_W)
        keys = turned(k_in[at, :].astype(f32), k_gain, b)
        keys = jnp.where(odd == 1, pltpu.roll(keys, head, 1), keys)
        values = v_in[at, :].astype(f32)
        values = jnp.where(odd == 1, values, pltpu.roll(values, head, 1))
        pair_ref[at, :] = jnp.where(first, keys, values).astype(bf16)
    own = pltpu.make_async_copy(
        outgo_ref.at[slot_rows(ep)], arrived.at[tp, slot_rows(ep)], loc_sem.at[0]
    )
    own.start()
    pl.semaphore_wait(barrier, n_ep - 1 + ny - 1 + 1)

    disp = [
        remote(outgo_ref.at[slot_rows(ep_at(d))], arrived.at[tp, slot_rows(ep)],
               disp_s.at[d], disp_r.at[d], ep_at(d), tp)
        for d in range(1, n_ep)
    ]
    nz = n_ep // 2
    side = lax.rem(ep, 2)
    col = ep // 2
    mate = col * 2 + 1 - side

    def col_from(d, which):
        return lax.rem(col - d + nz, nz) * 2 + which

    def kv_direct(d):
        return remote(pair_ref, kvbuf.at[ep], kv_s.at[d], kv_r.at[d],
                      lax.rem(col + d, nz) * 2 + side, tp)

    def kv_pass(d):
        held = kvbuf.at[col_from(d, side)]
        return remote(held, held, kv_s.at[nz + d], kv_r.at[nz + d], mate, tp)

    kv_mate = remote(pair_ref, kvbuf.at[ep], kv_s.at[nz], kv_r.at[nz], mate, tp)
    kv_mate.start()
    for copy in disp:
        copy.start()
    for d in range(1, nz):
        kv_direct(d).start()
    for copy in loads:
        copy.start()
    ins[4].start()

    ins[3].wait()
    for g in range(max(1, heads // 2)):
        for b in range(blocks):
            at = slice(b * GRID_W, (b + 1) * GRID_W)
            if heads == 1:
                values = q_in[at, :].astype(f32)
                values = jnp.concatenate([values, jnp.zeros_like(values)], axis=1)
            else:
                values = q_in[at, g * lane_count : (g + 1) * lane_count].astype(f32)
            values = turned(values, q_gain, b) * (head ** (-0.5))
            for h in range(min(2, heads)):
                part = values if h == 0 else pltpu.roll(values, head, 1)
                row_at = (2 * g + h) * rows_kv + b * GRID_W
                q_ref[row_at : row_at + GRID_W, :] = jnp.where(first, part, 0.0).astype(bf16)

    q_rows = q_ref.shape[0]
    tile = min(512, q_rows // 2)

    def attend(keys_of, first):
        keys = keys_of[...]
        lanes = lax.broadcasted_iota(jnp.int32, keys.shape, 1)
        kt[...] = keys.T
        vx[...] = jnp.where(lanes < keys.shape[1] // 2, jnp.ones_like(keys), keys)

        def one(i, carry):
            for sub in range(2):
                at = pl.ds(pl.multiple_of(i * 2 * tile + sub * tile, tile), tile)
                scores = jnp.dot(q_ref[at, :], kt[...], preferred_element_type=jnp.float32)
                weights = jnp.exp(scores).astype(jnp.bfloat16)
                term = jnp.dot(weights, vx[...], preferred_element_type=jnp.float32)
                if first:
                    acc[at, :] = term
                else:
                    acc[at, :] += term
            return carry

        lax.fori_loop(0, q_rows // (2 * tile), one, 0)

    attend(pair_ref, True)

    kv_mate.wait_recv()
    attend(kvbuf.at[mate], False)

    def later(d, carry):
        kv_direct(d).wait_recv()
        kv_pass(d).start()
        attend(kvbuf.at[col_from(d, side)], False)
        kv_pass(d).wait_recv()
        attend(kvbuf.at[col_from(d, 1 - side)], False)
        return carry

    early = 1 + (nz - 1) // 3
    late = max(early, nz - 1)
    lax.fori_loop(1, early, later, 0)

    own.wait()
    for copy in disp:
        copy.wait_recv()
    relay = [
        remote(arrived.at[tp], arrived.at[tp], rel_s.at[d], rel_r.at[d], ep, same_core(d))
        for d in range(1, ny)
    ]
    cross = [
        remote(arrived.at[row_from(d) * 2 + core], arrived.at[row_from(d) * 2 + core],
               fwd_s.at[d], rel_r.at[ny + d], ep, partner)
        for d in range(ny)
    ]
    for copy in relay:
        copy.start()
    cross[0].start()
    lax.fori_loop(early, late, later, 0)
    for d in range(1, ny):
        relay[d - 1].wait_recv()
        cross[d].start()
    lax.fori_loop(late, nz, later, 0)

    ins[4].wait()
    tokens = q_rows // heads
    half = acc.shape[1] // 2
    for j in range(n_tp):
        pieces = []
        for h in range(heads):
            a = acc[h * tokens + j * piece : h * tokens + (j + 1) * piece, :]
            pieces.append((a[:, half:] / a[:, :half]).astype(jnp.bfloat16))
        mine = pieces[0] if heads == 1 else jnp.concatenate(pieces, axis=1)
        pa[j % 2, j // 2] = jnp.dot(
            mine, wout_ref[...], preferred_element_type=jnp.float32
        ).astype(jnp.bfloat16)
    a1 = remote(pa.at[1 - core], pa_in, a1_s.at[0], a1_r.at[0], ep, partner)
    a1.start()

    for copy in cross:
        copy.wait_recv()
    loads[0].wait()
    loads[1].wait()
    a1.wait_recv()
    for y in range(ny):
        pa_red[y] = (
            pa[core, y].astype(jnp.float32) + pa_in[y].astype(jnp.float32)
        ).astype(jnp.bfloat16)
    a2 = [
        remote(pa_red.at[lax.rem(row + d, ny)], pa_in2.at[row],
               a2_s.at[d], a2_r.at[d], ep, same_core(d))
        for d in range(1, ny)
    ]
    for copy in a2:
        copy.start()

    ff = hidden.shape[1]
    step = min(256, ff)

    def gated(i, carry):
        at = pl.ds(pl.multiple_of(i * step, step), step)
        gate = jnp.zeros((slots, step), jnp.float32)
        up = jnp.zeros((slots, step), jnp.float32)
        for q in range(n_tp):
            x = arrived[q]
            gate = gate + jnp.dot(x, wg[q * dq : (q + 1) * dq, at], preferred_element_type=jnp.float32)
            up = up + jnp.dot(x, wu[q * dq : (q + 1) * dq, at], preferred_element_type=jnp.float32)
        hidden[:, at] = (gate / (1.0 + jnp.exp(-gate)) * up).astype(jnp.bfloat16)
        return carry

    lax.fori_loop(0, ff // step, gated, 0)
    loads[2].wait()

    def down_for(which):
        def down(y, carry):
            cols = pl.ds(pl.multiple_of((y * 2 + which) * dq, dq), dq)
            pm[which, y] = jnp.dot(
                hidden[...], wd[:, cols], preferred_element_type=jnp.float32
            ).astype(jnp.bfloat16)
            return carry

        lax.fori_loop(0, ny, down, 0)

    m1 = remote(pm.at[1 - core], pm_in, m1_s.at[0], m1_r.at[0], ep, partner)
    down_for(1 - core)
    m1.start()
    down_for(core)
    m1.wait_recv()
    for y in range(ny):
        pm_red[y] = (
            pm[core, y].astype(jnp.float32) + pm_in[y].astype(jnp.float32)
        ).astype(jnp.bfloat16)
    m2 = [
        remote(pm_red.at[lax.rem(row + d, ny)], pm_in2.at[row],
               m2_s.at[d], m2_r.at[d], ep, same_core(d))
        for d in range(1, ny)
    ]
    for copy in m2:
        copy.start()

    for copy in a2:
        copy.wait_recv()
    mixed = pa_red[row].astype(jnp.float32)
    for d in range(1, ny):
        mixed = mixed + pa_in2[row_from(d)].astype(jnp.float32)
    square = jnp.mean(mixed * mixed, axis=-1, keepdims=True)
    attn_ref[...] = (mixed * lax.rsqrt(square + EPSILON) * gain_ref[...]).astype(jnp.bfloat16)

    for copy in m2:
        copy.wait_recv()
    total = pm_red[row].astype(jnp.float32)
    for d in range(1, ny):
        total = total + pm_in2[row_from(d)].astype(jnp.float32)
    summed[...] = total.astype(jnp.bfloat16)
    back = [
        remote(summed.at[slot_rows(ep_at(d))], ret.at[slot_rows(ep)],
               ret_s.at[d], ret_r.at[d], ep_at(d), tp)
        for d in range(1, n_ep)
    ]
    for copy in back:
        copy.start()
    mine = pltpu.make_async_copy(
        summed.at[slot_rows(ep)], ret.at[slot_rows(ep)], loc_sem.at[1]
    )
    mine.start()
    mine.wait()
    for copy in back:
        copy.wait_recv()
    mixw = mixw_ref[...]
    high = mixw.astype(jnp.bfloat16)
    low = (mixw - high.astype(jnp.float32)).astype(jnp.bfloat16)
    over = (((0,), (0,)), ((), ()))
    moe_ref[...] = (
        lax.dot_general(high, ret[...], over, preferred_element_type=jnp.float32)
        + lax.dot_general(low, ret[...], over, preferred_element_type=jnp.float32)
    ).astype(jnp.bfloat16)

    for copy in [kv_mate] + disp + relay + cross + [a1] + a2 + [m1] + m2 + back:
        copy.wait_send()

    def kv_done(d, carry):
        kv_direct(d).wait_send()
        kv_pass(d).wait_send()
        return carry

    lax.fori_loop(1, nz, kv_done, 0)


def per_device(
    n_ep, n_tp,
    q_in, k_in, v_in, q_gain, k_gain, w_out, post_gain,
    moe_in, routes, route_logits, pre_gain, w_gate, w_up, w_down,
):
    bf16 = jnp.bfloat16
    head = q_gain.shape[0]
    rows = q_in.shape[0]
    heads = q_in.shape[1] // head
    kv_count = k_in.shape[1] // head
    repeat = heads * n_tp // kv_count
    ny = n_tp // 2
    grid_rows = turn_tables(n_ep * rows, GRID_W, head // 4)

    tokens, top = routes.shape
    width = moe_in.shape[1]
    dq = width // n_tp
    need = max(2, 3 * top * tokens // (2 * n_ep))
    cap = -(-need // 16) * 16
    slots = n_ep * cap

    piece = rows // n_tp
    ff = w_gate.shape[2]
    dma = pltpu.SemaphoreType.DMA
    vmem = pl.BlockSpec(memory_space=pltpu.VMEM)
    hbm = pl.BlockSpec(memory_space=pl.ANY)
    return pl.pallas_call(
        functools.partial(kernel, (n_ep, n_tp, heads, cap, repeat)),
        out_shape=(
            jax.ShapeDtypeStruct((piece, width), bf16),
            jax.ShapeDtypeStruct((tokens, dq), bf16),
        ),
        in_specs=[vmem] * 10 + [hbm] * 8,
        out_specs=(vmem, vmem),
        scratch_shapes=[
            pltpu.VMEM((rows, heads * head), bf16),
            pltpu.VMEM((rows, 2 * head), bf16),
            pltpu.VMEM((rows, 2 * head), bf16),
            pltpu.VMEM((tokens, width), bf16),
            pltpu.VMEM((heads * head, width), bf16),
            pltpu.VMEM((heads * rows, 2 * head), bf16),
            pltpu.VMEM((rows, 2 * head), bf16),
            pltpu.VMEM((slots, tokens), bf16),
            pltpu.VMEM((slots, dq), bf16),
            pltpu.VMEM((slots, tokens), jnp.float32),
            pltpu.VMEM((width, ff), bf16),
            pltpu.VMEM((width, ff), bf16),
            pltpu.VMEM((ff, width), bf16),
            pltpu.VMEM((n_ep, rows, 2 * head), bf16),
            pltpu.VMEM((rows, 2 * head), bf16),
            pltpu.VMEM((2 * head, rows), bf16),
            pltpu.VMEM((heads * rows, 2 * head), jnp.float32),
            pltpu.VMEM((n_tp, slots, dq), bf16),
            pltpu.VMEM((slots, ff), bf16),
            pltpu.VMEM((2, ny, piece, width), bf16),
            pltpu.VMEM((ny, piece, width), bf16),
            pltpu.VMEM((ny, piece, width), bf16),
            pltpu.VMEM((ny, piece, width), bf16),
            pltpu.VMEM((2, ny, slots, dq), bf16),
            pltpu.VMEM((ny, slots, dq), bf16),
            pltpu.VMEM((ny, slots, dq), bf16),
            pltpu.VMEM((ny, slots, dq), bf16),
            pltpu.VMEM((slots, dq), bf16),
            pltpu.VMEM((slots, dq), bf16),
            dma((5,)), dma((3,)), dma((2,)),
            dma((n_ep,)), dma((n_ep,)), dma((n_ep,)), dma((n_ep,)),
            dma((ny,)), dma((2 * ny,)), dma((ny,)),
            dma((1,)), dma((1,)), dma((ny,)), dma((ny,)),
            dma((1,)), dma((1,)), dma((ny,)), dma((ny,)),
            dma((n_ep,)), dma((n_ep,)),
        ],
        compiler_params=pltpu.CompilerParams(
            collective_id=0, has_side_effects=True, vmem_limit_bytes=60 * 1024 * 1024
        ),
    )(
        routes.T, route_logits.T, pre_gain[None, :], post_gain[None, :], q_gain[None, :], k_gain[None, :], *grid_rows,
        q_in, k_in, v_in, moe_in, w_out, w_gate[0], w_up[0], w_down[0],
    )


def solution(mesh):
    return jax.shard_map(
        functools.partial(per_device, mesh.shape["ep"], mesh.shape["tp"]),
        mesh=mesh,
        in_specs=(
            P("ep", "tp"),
            P("ep", None),
            P("ep", None),
            P(),
            P(),
            P("tp", None),
            P(),
            P("ep", None),
            P("ep", None),
            P("ep", None),
            P(),
            P("ep", None, "tp"),
            P("ep", None, "tp"),
            P("ep", "tp", None),
        ),
        out_specs=(P(("ep", "tp"), None), P("ep", "tp")),
        check_vma=False,
    )
```

```python
import functools

import jax
import jax.numpy as jnp
import numpy as np
from jax import lax
from jax.experimental import pallas as pl
from jax.experimental.pallas import tpu as pltpu
from jax.sharding import PartitionSpec as P

GRID_W = 128
EPSILON = 1e-06
ROPE_BASE = 10000.0
MESH = pl.DeviceIdType.MESH


def turn_tables(positions, rows_of_grid, quarter):
    inverse = ROPE_BASE ** (-np.arange(quarter, dtype=np.float32) / np.float32(quarter))
    inverse = inverse.astype(np.float32)

    def table(count, first_half):
        angles = (np.arange(count, dtype=np.float32)[:, None] * inverse[None, :]).astype(np.float64)
        cos, sin = np.cos(angles), np.sin(angles)
        none = np.zeros_like(cos)
        cos = np.concatenate([cos, cos, none, none] if first_half else [none, none, cos, cos], axis=1)
        sin = np.concatenate([-sin, sin, none, none] if first_half else [none, none, -sin, sin], axis=1)
        return np.concatenate([cos, cos], axis=1), np.concatenate([sin, sin], axis=1)

    grid_rows = positions // rows_of_grid
    by_row = table(grid_rows, True)
    by_col = table(rows_of_grid, False)
    return [jnp.asarray(part, jnp.float32) for part in by_row + by_col]


def kernel(
    dims,
    route_ref, logit_ref, pre_ref, gain_ref, qg_ref, kg_ref, crow_ref, srow_ref, ccol_ref, scol_ref,
    q_hbm, k_hbm, v_hbm, x_hbm, wout_hbm, wg_hbm, wu_hbm, wd_hbm,
    attn_ref, moe_ref,
    q_in, k_in, v_in, x_ref, wout_ref, q_ref, placed_ref,
    outgo_ref, mixw_ref, wg, wu, wd, kvbuf, vx, kt, acc, arrived, hidden,
    pa, pa_in, pa_red, pa_in2, pm, pm_in, pm_red, pm_in2, summed, ret,
    in_sem, w_sem, kz_s, kz_r, kx_s, kx_r, disp_s, disp_r, rel_s, rel_r, c0_s, c0_r, cy_s, cy_r,
    a1_s, a1_r, a2_s, a2_r, m1_s, m1_r, m2_s, m2_r, ret_s, ret_r,
):
    n_ep, n_tp, heads, cap, repeat = dims
    ny = n_tp // 2
    nz = n_ep // 2
    ep = lax.axis_index("ep")
    tp = lax.axis_index("tp")
    core = lax.rem(tp, 2)
    row = lax.div(tp, 2)
    partner = row * 2 + 1 - core
    side = lax.rem(ep, 2)
    col = lax.div(ep, 2)
    mate = col * 2 + 1 - side
    rows_kv = k_in.shape[0]
    dq = outgo_ref.shape[1]
    slots = outgo_ref.shape[0]
    piece = attn_ref.shape[0]
    bf16, f32 = jnp.bfloat16, jnp.float32

    def remote(src, dst, ss, rs, e, t):
        return pltpu.make_async_remote_copy(
            src_ref=src, dst_ref=dst, send_sem=ss, recv_sem=rs,
            device_id=(e, t), device_id_type=MESH,
        )

    def wait(name, copy):
        with jax.named_scope(name):
            copy.wait_recv()

    def ep_at(d):
        return lax.rem(ep + d, n_ep)

    def flip(d):
        other = ep
        for bit in range(n_ep.bit_length() - 1):
            if (d >> bit) % 2:
                other = other + (1 << bit) * (1 - 2 * lax.rem(lax.div(ep, 1 << bit), 2))
        return other

    def same_core(d):
        return lax.rem(row + d, ny) * 2 + core

    def row_from(d):
        return lax.rem(row - d + ny, ny)

    def slot_rows(e):
        return pl.ds(pl.multiple_of(e * cap, cap), cap)

    def lanes_of(t):
        return pl.ds(pl.multiple_of(t * dq, dq), dq)

    quarter = n_ep // 4
    near = list(range(quarter - 1, -1, -1))
    groups = [
        list(range(2 * quarter, 3 * quarter)) + near,
        list(range(3 * quarter, 4 * quarter)) + list(range(quarter, 2 * quarter)),
    ]
    order = groups[0] + groups[1]
    chunk = slots // 2
    part = chunk // 2

    def held(d):
        return pl.ds(order.index(d) * cap, cap)

    head = qg_ref.shape[1]
    lane_count = 2 * head
    kv_index = lax.div(tp * heads, repeat)
    kv_lanes = pl.ds(pl.multiple_of(lax.div(kv_index, 2) * lane_count, lane_count), lane_count)
    ins = [
        pltpu.make_async_copy(src, dst, in_sem.at[i])
        for i, (src, dst) in enumerate((
            (x_hbm, x_ref), (k_hbm.at[:, kv_lanes], k_in), (v_hbm.at[:, kv_lanes], v_in),
            (q_hbm, q_in), (wout_hbm, wout_ref),
        ))
    ]
    for copy in ins[:4]:
        copy.start()
    loads = [
        pltpu.make_async_copy(src, dst, w_sem.at[i])
        for i, (src, dst) in enumerate(((wg_hbm, wg), (wu_hbm, wu), (wd_hbm, wd)))
    ]
    barrier = pltpu.get_barrier_semaphore()
    for d in range(1, n_ep):
        pl.semaphore_signal(barrier, inc=1, device_id=(ep_at(d), tp), device_id_type=MESH)
    for d in range(1, ny):
        pl.semaphore_signal(barrier, inc=1, device_id=(ep, same_core(d)), device_id_type=MESH)
    pl.semaphore_signal(barrier, inc=1, device_id=(ep, partner), device_id_type=MESH)

    top, tokens = logit_ref.shape
    logits = logit_ref[...]
    power = jnp.exp(logits - jnp.max(logits, axis=0, keepdims=True))
    chance = power / jnp.sum(power, axis=0, keepdims=True)
    expert = lax.broadcasted_iota(jnp.int32, (n_ep, tokens), 0)
    named = jnp.zeros((n_ep, tokens), f32)
    share = jnp.zeros((n_ep, tokens), f32)
    for j in range(top):
        hit = route_ref[j : j + 1, :] == expert
        named = jnp.where(hit, 1.0, named)
        share = jnp.where(hit, chance[j : j + 1, :], share)
    above = lax.broadcasted_iota(jnp.int32, (tokens, tokens), 0) < lax.broadcasted_iota(
        jnp.int32, (tokens, tokens), 1
    )
    rank = jnp.dot(named, jnp.where(above, 1.0, 0.0), preferred_element_type=f32)
    rank = jnp.where(named > 0.0, rank, -1.0)
    place = lax.broadcasted_iota(jnp.int32, (cap, tokens), 0).astype(f32)
    for e in range(n_ep):
        there = rank[e : e + 1, :] == place
        placed_ref[e * cap : (e + 1) * cap, :] = jnp.where(there, 1.0, 0.0).astype(bf16)
        mixw_ref[e * cap : (e + 1) * cap, :] = jnp.where(there, share[e : e + 1, :], 0.0)

    ins[0].wait()
    x = x_ref[...].astype(f32)
    scale = lax.rsqrt(jnp.mean(x * x, axis=-1, keepdims=True) + EPSILON)
    mine = pl.ds(pl.multiple_of(tp * dq, dq), dq)
    normed = (x_ref[:, mine].astype(f32) * scale * pre_ref[:, mine]).astype(bf16)
    outgo_ref[...] = jnp.dot(placed_ref[...], normed, preferred_element_type=f32).astype(bf16)

    lane = lax.broadcasted_iota(jnp.int32, (GRID_W, lane_count), 1)
    first = lane < head
    ahead = lax.rem(lane, head // 2) < head // 4
    joined = lax.broadcasted_iota(jnp.int32, (lane_count, lane_count), 0) // head == (
        lax.broadcasted_iota(jnp.int32, (lane_count, lane_count), 1) // head
    )
    joined = jnp.where(joined, 1.0, 0.0).astype(bf16)
    blocks = rows_kv // GRID_W

    def turned(values, gain, b):
        square = values * values
        high = square.astype(bf16)
        low = (square - high.astype(f32)).astype(bf16)
        total = jnp.dot(high, joined, preferred_element_type=f32) + jnp.dot(
            low, joined, preferred_element_type=f32
        )
        values = values * lax.rsqrt(total * (1.0 / head) + EPSILON) * gain
        other = jnp.where(
            ahead,
            pltpu.roll(values, lane_count - head // 4, 1),
            pltpu.roll(values, head // 4, 1),
        )
        at = pl.ds(ep * blocks + b, 1)
        return values * (crow_ref[at, :] + ccol_ref[...]) + other * (srow_ref[at, :] + scol_ref[...])

    k_gain = jnp.concatenate([kg_ref[...], kg_ref[...]], axis=1)
    q_gain = jnp.concatenate([qg_ref[...], qg_ref[...]], axis=1)
    odd = lax.rem(kv_index, 2)
    ins[1].wait()
    ins[2].wait()
    for b in range(blocks):
        at = slice(b * GRID_W, (b + 1) * GRID_W)
        keys = turned(k_in[at, :].astype(f32), k_gain, b)
        keys = jnp.where(odd == 1, pltpu.roll(keys, head, 1), keys)
        values = v_in[at, :].astype(f32)
        values = jnp.where(odd == 1, values, pltpu.roll(values, head, 1))
        kvbuf[ep, at, :] = jnp.where(first, keys, values).astype(bf16)
    with jax.named_scope("barrier"):
        pl.semaphore_wait(barrier, n_ep - 1 + ny - 1 + 1)

    disp = {
        d: remote(outgo_ref.at[slot_rows(flip(d))], arrived.at[held(d), lanes_of(tp)],
                  disp_s.at[d], disp_r.at[d], flip(d), tp)
        for d in range(1, n_ep)
    }

    def kv_line(b, target, sem):
        block = kvbuf.at[b * 2 + side]
        return remote(block, block, kz_s.at[sem], kz_r.at[b], target * 2 + side, tp)

    def kv_pass(b):
        block = kvbuf.at[b * 2 + side]
        return remote(block, block, kx_s.at[b], kx_r.at[b], mate, tp)

    has_next = col < nz - 1
    has_prev = col > 0

    kv_pass(col).start()
    for d in groups[0]:
        if d:
            disp[d].start()

    @pl.when(has_next)
    def _():
        kv_line(col, col + 1, col).start()

    @pl.when(has_prev)
    def _():
        kv_line(col, col - 1, nz).start()

    for d in groups[1]:
        disp[d].start()
    for copy in loads:
        copy.start()
    ins[4].start()

    ins[3].wait()
    for g in range(max(1, heads // 2)):
        for b in range(blocks):
            at = slice(b * GRID_W, (b + 1) * GRID_W)
            if heads == 1:
                values = q_in[at, :].astype(f32)
                values = jnp.concatenate([values, jnp.zeros_like(values)], axis=1)
            else:
                values = q_in[at, g * lane_count : (g + 1) * lane_count].astype(f32)
            values = turned(values, q_gain, b) * (head ** (-0.5))
            for h in range(min(2, heads)):
                one = values if h == 0 else pltpu.roll(values, head, 1)
                one = jnp.where(first, one, 0.0).astype(bf16)
                for i in range(max(1, GRID_W // piece)):
                    size = min(piece, GRID_W)
                    token = b * GRID_W + i * size
                    row_at = (token // piece * heads + 2 * g + h) * piece + token % piece
                    q_ref[row_at : row_at + size, :] = one[i * size : (i + 1) * size, :]

    mine_rows = placed_ref[slot_rows(ep), :]
    for q in range(n_tp):
        at = slice(q * dq, (q + 1) * dq)
        full = (x_ref[:, at].astype(f32) * scale * pre_ref[:, at]).astype(bf16)
        arrived[held(0), at] = jnp.dot(mine_rows, full, preferred_element_type=f32).astype(bf16)

    q_rows = q_ref.shape[0]
    tile = min(512, heads * piece)

    def prepare(e, slot):
        keys = kvbuf[e]
        lanes = lax.broadcasted_iota(jnp.int32, keys.shape, 1)
        kt[slot] = keys.T
        vx[slot] = jnp.where(lanes < keys.shape[1] // 2, jnp.ones_like(keys), keys)

    def attend_rows(i, slot, fresh):
        for sub in range(2):
            at = pl.ds(pl.multiple_of(i * 2 * tile + sub * tile, tile), tile)
            scores = jnp.dot(q_ref[at, :], kt[slot], preferred_element_type=f32)
            weights = jnp.exp(scores).astype(bf16)
            term = jnp.dot(weights, vx[slot], preferred_element_type=f32)
            if fresh:
                acc[at, :] = term
            else:
                acc[at, :] += term

    def attend(e, fresh):
        prepare(e, 0)

        def one(i, carry):
            attend_rows(i, 0, fresh)
            return carry

        lax.fori_loop(0, q_rows // (2 * tile), one, 0)

    shorter = jnp.minimum(col, nz - 1 - col)
    longer = jnp.where(col <= nz - 1 - col, 1, -1)

    def line_step(k):
        both = k < 2 * shorter
        way = jnp.where(both, 2 * lax.rem(k, 2) - 1, longer)
        far = jnp.where(both, lax.div(k, 2) + 1, k - shorter + 1)
        return col + way * far, col - way

    def line_one(k):
        b, target = line_step(k)
        wait("kv_line", kv_line(b, target, b))

        @pl.when(jnp.logical_and(target >= 0, target <= nz - 1))
        def _():
            kv_line(b, target, b).start()

        kv_pass(b).start()

    def line_take(k):
        both = k < 2 * shorter
        opening = jnp.logical_or(lax.rem(k, 2) == 0, jnp.logical_not(both))

        @pl.when(opening)
        def _():
            line_one(k)

        @pl.when(jnp.logical_and(opening, both))
        def _():
            line_one(k + 1)

    def line_block(k):
        return line_step(k)[0] * 2 + side

    def pass_block(k):
        b, _ = line_step(k)
        wait("kv_pass", kv_pass(b))
        return b * 2 + 1 - side

    def take(k, carry):
        line_take(k)
        attend(line_block(k), False)
        attend(pass_block(k), False)
        return carry

    def relay(d, dy):
        block = arrived.at[held(d), lanes_of(tp)]
        return remote(block, block, rel_s.at[d, dy], rel_r.at[d, dy], ep, same_core(dy))

    def foreign(c):
        count = len(groups[c]) - (1 if 0 in groups[c] else 0)
        return pl.ds(c * chunk, count * cap)

    def cross(c, dy):
        block = arrived.at[foreign(c), lanes_of(row_from(dy) * 2 + core)]
        if dy == 0:
            return remote(block, block, c0_s.at[c], c0_r.at[c], ep, partner)
        return remote(block, block, cy_s.at[c, dy], cy_r.at[c, dy], ep, partner)

    def relay_chunk(c):
        for d in groups[c]:
            if d:
                wait("disp", disp[d])
                for dy in range(1, ny):
                    relay(d, dy).start()
        cross(c, 0).start()

    def cross_chunk(c):
        for dy in range(1, ny):
            for d in groups[c]:
                if d:
                    wait("relay", relay(d, dy))
            cross(c, dy).start()

    ff = hidden.shape[1]
    step = min(256, ff)

    def m1(c):
        return remote(pm.at[c, 1 - core], pm_in.at[c], m1_s.at[c], m1_r.at[c], ep, partner)

    def m2(c, s, dy):
        at = pl.ds(s * part, part)
        return remote(pm_red.at[c, lax.rem(row + dy, ny), at], pm_in2.at[c, row, at],
                      m2_s.at[c, s, dy], m2_r.at[c, s, dy], ep, same_core(dy))

    def experts(c):
        for dy in range(ny):
            wait("cross", cross(c, dy))
        if c == 0:
            loads[0].wait()
            loads[1].wait()
        rows = slice(c * chunk, (c + 1) * chunk)

        def gated(i, carry):
            at = pl.ds(pl.multiple_of(i * step, step), step)
            x = arrived[rows, :]
            gate = jnp.dot(x, wg[:, at], preferred_element_type=f32)
            up = jnp.dot(x, wu[:, at], preferred_element_type=f32)
            hidden[rows, at] = (gate / (1.0 + jnp.exp(-gate)) * up).astype(bf16)
            return carry

        lax.fori_loop(0, ff // step, gated, 0)
        if c == 0:
            loads[2].wait()

        def down_for(which):
            def down(y, carry):
                cols = pl.ds(pl.multiple_of((y * 2 + which) * dq, dq), dq)
                pm[c, which, y] = jnp.dot(
                    hidden[rows, :], wd[:, cols], preferred_element_type=f32
                ).astype(bf16)
                return carry

            lax.fori_loop(0, ny, down, 0)

        down_for(1 - core)
        m1(c).start()
        down_for(core)

    def reduce_cores(c):
        wait("m1", m1(c))
        for y in range(ny):
            pm_red[c, y] = (pm[c, core, y].astype(f32) + pm_in[c, y].astype(f32)).astype(bf16)
        for s in range(2):
            for dy in range(1, ny):
                m2(c, s, dy).start()

    def back(d):
        return remote(summed.at[held(d)], ret.at[slot_rows(ep)], ret_s.at[d], ret_r.at[d], flip(d), tp)

    def send_back(c):
        for s in range(2):
            for dy in range(1, ny):
                wait("m2", m2(c, s, dy))
            at = slice(s * part, (s + 1) * part)
            total = pm_red[c, row, at].astype(f32)
            for dy in range(1, ny):
                total = total + pm_in2[c, row_from(dy), at].astype(f32)
            total = total.astype(bf16)
            rows_at = c * chunk + s * part
            summed[rows_at : rows_at + part, :] = total
            for d in order[rows_at // cap : (rows_at + part) // cap]:
                if d:
                    back(d).start()
                else:
                    low = order.index(0) * cap - rows_at
                    ret[slot_rows(ep), :] = total[low : low + cap, :]

    tall = heads * piece
    half = acc.shape[1] // 2

    def finish(target):
        for slot in range(2):
            for i in range(2 * tall // (2 * tile)):
                attend_rows(target * (tall // tile) + i, slot, False)
        sides = []
        for c in range(2):
            which = core if c else 1 - core
            pieces = []
            for h in range(heads):
                at = pl.ds(pl.multiple_of((target * 2 + which) * tall + h * piece, piece), piece)
                sums = acc[at, :]
                pieces.append((sums[:, half:] / sums[:, :half]).astype(bf16))
            sides.append(pieces[0] if heads == 1 else jnp.concatenate(pieces, axis=1))
        both = jnp.concatenate(sides, axis=0)
        return jnp.dot(both, wout_ref[...], preferred_element_type=f32)

    def a1(d):
        return remote(pa.at[d], pa_in.at[d], a1_s.at[d], a1_r.at[d], ep, partner)

    def a2(d):
        return remote(pa_red.at[d], pa_in2.at[d], a2_s.at[d], a2_r.at[d], ep, same_core(d))

    def finish_start(d):
        total = finish(lax.rem(row + d, ny)).astype(bf16)
        pa[d] = total[:piece]
        a1(d).start()
        pa_red[d] = total[piece:]

    def finish_end(d):
        wait("a1", a1(d))
        return pa_red[d].astype(f32) + pa_in[d].astype(f32)

    attend(ep, True)
    wait("kv_mate", kv_pass(col))
    attend(mate, False)
    relay_chunk(0)
    split = max(1, (nz - 1) // 2)
    line_take(0)
    attend(line_block(0), False)
    relay_chunk(1)
    attend(pass_block(0), False)
    lax.fori_loop(1, split, take, 0)
    cross_chunk(0)
    line_take(split)
    attend(line_block(split), False)
    with jax.named_scope("experts0"):
        experts(0)
    cross_chunk(1)
    attend(pass_block(split), False)
    reduce_cores(0)
    lax.fori_loop(split + 1, nz - 2, take, 0)
    line_take(nz - 2)
    prepare(line_block(nz - 2), 0)
    with jax.named_scope("experts1"):
        experts(1)
    send_back(0)
    prepare(pass_block(nz - 2), 1)
    ins[4].wait()
    reduce_cores(1)
    for d in range(1, ny):
        with jax.named_scope("finish_other"):
            finish_start(d)
    for d in range(1, ny):
        pa_red[d] = finish_end(d).astype(bf16)
        a2(d).start()
    send_back(1)
    with jax.named_scope("finish_own"):
        finish_start(0)
    mixed = finish_end(0).astype(bf16).astype(f32)
    for d in range(1, ny):
        wait("a2", a2(d))
        mixed = mixed + pa_in2[d].astype(f32)
    square = jnp.mean(mixed * mixed, axis=-1, keepdims=True)
    attn_ref[...] = (mixed * lax.rsqrt(square + EPSILON) * gain_ref[...]).astype(bf16)

    for d in range(1, n_ep):
        wait("back", back(d))
    mixw = mixw_ref[...]
    high = mixw.astype(bf16)
    low = (mixw - high.astype(f32)).astype(bf16)
    over = (((0,), (0,)), ((), ()))
    moe_ref[...] = (
        lax.dot_general(high, ret[...], over, preferred_element_type=f32)
        + lax.dot_general(low, ret[...], over, preferred_element_type=f32)
    ).astype(bf16)

    sent = [kv_pass(col)] + list(disp.values())
    sent += [relay(d, dy) for d in range(1, n_ep) for dy in range(1, ny)]
    sent += [cross(c, dy) for c in range(2) for dy in range(ny)]
    sent += [m1(c) for c in range(2)]
    sent += [m2(c, s, dy) for c in range(2) for s in range(2) for dy in range(1, ny)]
    sent += [back(d) for d in range(1, n_ep)]
    sent += [a1(d) for d in range(ny)] + [a2(d) for d in range(1, ny)]
    for copy in sent:
        copy.wait_send()

    @pl.when(has_next)
    def _():
        kv_line(col, col + 1, col).wait_send()

    @pl.when(has_prev)
    def _():
        kv_line(col, col - 1, nz).wait_send()

    def kv_done(k, carry):
        b, target = line_step(k)

        @pl.when(jnp.logical_and(target >= 0, target <= nz - 1))
        def _():
            kv_line(b, target, b).wait_send()

        kv_pass(b).wait_send()
        return carry

    lax.fori_loop(0, nz - 1, kv_done, 0)


def per_device(
    n_ep, n_tp,
    q_in, k_in, v_in, q_gain, k_gain, w_out, post_gain,
    moe_in, routes, route_logits, pre_gain, w_gate, w_up, w_down,
):
    bf16 = jnp.bfloat16
    head = q_gain.shape[0]
    rows = q_in.shape[0]
    heads = q_in.shape[1] // head
    kv_count = k_in.shape[1] // head
    repeat = heads * n_tp // kv_count
    ny = n_tp // 2
    nz = n_ep // 2
    grid_rows = turn_tables(n_ep * rows, GRID_W, head // 4)

    tokens, top = routes.shape
    width = moe_in.shape[1]
    dq = width // n_tp
    need = max(2, 3 * top * tokens // (2 * n_ep))
    cap = -(-need // 16) * 16
    slots = n_ep * cap

    piece = rows // n_tp
    ff = w_gate.shape[2]
    dma = pltpu.SemaphoreType.DMA
    vmem = pl.BlockSpec(memory_space=pltpu.VMEM)
    hbm = pl.BlockSpec(memory_space=pl.ANY)
    return pl.pallas_call(
        functools.partial(kernel, (n_ep, n_tp, heads, cap, repeat)),
        out_shape=(
            jax.ShapeDtypeStruct((piece, width), bf16),
            jax.ShapeDtypeStruct((tokens, dq), bf16),
        ),
        in_specs=[vmem] * 10 + [hbm] * 8,
        out_specs=(vmem, vmem),
        scratch_shapes=[
            pltpu.VMEM((rows, heads * head), bf16),
            pltpu.VMEM((rows, 2 * head), bf16),
            pltpu.VMEM((rows, 2 * head), bf16),
            pltpu.VMEM((tokens, width), bf16),
            pltpu.VMEM((heads * head, width), bf16),
            pltpu.VMEM((heads * rows, 2 * head), bf16),
            pltpu.VMEM((slots, tokens), bf16),
            pltpu.VMEM((slots, dq), bf16),
            pltpu.VMEM((slots, tokens), jnp.float32),
            pltpu.VMEM((width, ff), bf16),
            pltpu.VMEM((width, ff), bf16),
            pltpu.VMEM((ff, width), bf16),
            pltpu.VMEM((n_ep, rows, 2 * head), bf16),
            pltpu.VMEM((2, rows, 2 * head), bf16),
            pltpu.VMEM((2, 2 * head, rows), bf16),
            pltpu.VMEM((heads * rows, 2 * head), jnp.float32),
            pltpu.VMEM((slots, width), bf16),
            pltpu.VMEM((slots, ff), bf16),
            pltpu.VMEM((ny, piece, width), bf16),
            pltpu.VMEM((ny, piece, width), bf16),
            pltpu.VMEM((ny, piece, width), bf16),
            pltpu.VMEM((ny, piece, width), bf16),
            pltpu.VMEM((2, 2, ny, slots // 2, dq), bf16),
            pltpu.VMEM((2, ny, slots // 2, dq), bf16),
            pltpu.VMEM((2, ny, slots // 2, dq), bf16),
            pltpu.VMEM((2, ny, slots // 2, dq), bf16),
            pltpu.VMEM((slots, dq), bf16),
            pltpu.VMEM((slots, dq), bf16),
            dma((5,)), dma((3,)),
            dma((nz + 1,)), dma((nz,)), dma((nz,)), dma((nz,)),
            dma((n_ep,)), dma((n_ep,)), dma((n_ep, ny)), dma((n_ep, ny)),
            dma((2,)), dma((2,)), dma((2, ny)), dma((2, ny)),
            dma((ny,)), dma((ny,)), dma((ny,)), dma((ny,)),
            dma((2,)), dma((2,)), dma((2, 2, ny)), dma((2, 2, ny)),
            dma((n_ep,)), dma((n_ep,)),
        ],
        compiler_params=pltpu.CompilerParams(
            collective_id=0, has_side_effects=True, vmem_limit_bytes=60 * 1024 * 1024
        ),
    )(
        routes.T, route_logits.T, pre_gain[None, :], post_gain[None, :], q_gain[None, :], k_gain[None, :], *grid_rows,
        q_in, k_in, v_in, moe_in, w_out, w_gate[0], w_up[0], w_down[0],
    )


def solution(mesh):
    return jax.shard_map(
        functools.partial(per_device, mesh.shape["ep"], mesh.shape["tp"]),
        mesh=mesh,
        in_specs=(
            P("ep", "tp"),
            P("ep", None),
            P("ep", None),
            P(),
            P(),
            P("tp", None),
            P(),
            P("ep", None),
            P("ep", None),
            P("ep", None),
            P(),
            P("ep", None, "tp"),
            P("ep", None, "tp"),
            P("ep", "tp", None),
        ),
        out_specs=(P(("ep", "tp"), None), P("ep", "tp")),
        check_vma=False,
    )
```

```python
import functools

import jax
import jax.numpy as jnp
import numpy as np
from jax import lax
from jax.experimental import pallas as pl
from jax.experimental.pallas import tpu as pltpu
from jax.sharding import PartitionSpec as P

GRID_W = 128
EPSILON = 1e-06
ROPE_BASE = 10000.0
MESH = pl.DeviceIdType.MESH
SKEW = 128
VMEM_LIMIT = 60 * 1024 * 1024


def turn_tables(positions, rows_of_grid, quarter):
    inverse = ROPE_BASE ** (-np.arange(quarter, dtype=np.float32) / np.float32(quarter))
    inverse = inverse.astype(np.float32)

    def table(count, first_half):
        angles = (np.arange(count, dtype=np.float32)[:, None] * inverse[None, :]).astype(np.float64)
        cos, sin = np.cos(angles), np.sin(angles)
        none = np.zeros_like(cos)
        cos = np.concatenate([cos, cos, none, none] if first_half else [none, none, cos, cos], axis=1)
        sin = np.concatenate([-sin, sin, none, none] if first_half else [none, none, -sin, sin], axis=1)
        return np.concatenate([cos, cos], axis=1), np.concatenate([sin, sin], axis=1)

    grid_rows = positions // rows_of_grid
    by_row = table(grid_rows, True)
    by_col = table(rows_of_grid, False)
    return jnp.asarray(np.concatenate(by_row + by_col), jnp.float32)


def kernel(
    dims,
    route_hbm, logit_hbm, pre_hbm, gain_hbm, qg_hbm, kg_hbm, turn_hbm,
    q_hbm, k_hbm, v_hbm, x_hbm, wout_hbm, wg_hbm, wu_hbm, wd_hbm,
    attn_ref, moe_ref,
    route_ref, logit_ref, pre_ref, gain_ref, qg_ref, kg_ref, turn_ref,
    q_in, k_in, v_in, x_ref, wout_ref, q_ref, placed_ref,
    outgo_ref, mixw_ref, wg, wu, wd, kvbuf, vx, kt, acc, arrived, hidden,
    pa, pa_in, pa_red, pa_in2, pm, pm_in, pm_red, pm_in2, summed, ret,
    in_sem, w_sem, kz_s, kz_r, kx_s, kx_r, disp_s, disp_r, rel_s, rel_r, c0_s, c0_r, cy_s, cy_r,
    a1_s, a1_r, a2_s, a2_r, m1_s, m1_r, m2_s, m2_r, ret_s, ret_r,
):
    n_ep, n_tp, heads, cap, repeat = dims
    ny = n_tp // 2
    nz = n_ep // 2
    ep = lax.axis_index("ep")
    tp = lax.axis_index("tp")
    core = lax.rem(tp, 2)
    row = lax.div(tp, 2)
    partner = row * 2 + 1 - core
    side = lax.rem(ep, 2)
    col = lax.div(ep, 2)
    mate = col * 2 + 1 - side
    rows_kv = k_in.shape[0]
    dq = outgo_ref.shape[1]
    slots = outgo_ref.shape[0]
    piece = attn_ref.shape[0]
    bf16, f32 = jnp.bfloat16, jnp.float32

    def remote(src, dst, ss, rs, e, t):
        return pltpu.make_async_remote_copy(
            src_ref=src, dst_ref=dst, send_sem=ss, recv_sem=rs,
            device_id=(e, t), device_id_type=MESH,
        )

    def wait(name, copy):
        with jax.named_scope(name):
            copy.wait_recv()

    def ep_at(d):
        return lax.rem(ep + d, n_ep)

    def flip(d):
        other = ep
        for bit in range(n_ep.bit_length() - 1):
            if (d >> bit) % 2:
                other = other + (1 << bit) * (1 - 2 * lax.rem(lax.div(ep, 1 << bit), 2))
        return other

    def same_core(d):
        return lax.rem(row + d, ny) * 2 + core

    def row_from(d):
        return lax.rem(row - d + ny, ny)

    def slot_rows(e):
        return pl.ds(pl.multiple_of(e * cap, cap), cap)

    def cols_of(ref):
        return pl.ds(0, ref.shape[1])

    def lanes_of(t):
        return pl.ds(pl.multiple_of(t * dq, dq), dq)

    quarter = n_ep // 4
    near = list(range(quarter - 1, -1, -1))
    groups = [
        list(range(2 * quarter, 3 * quarter)) + near,
        list(range(3 * quarter, 4 * quarter)) + list(range(quarter, 2 * quarter)),
    ]
    order = groups[0] + groups[1]
    chunk = slots // 2
    part = chunk // 2

    def held(d):
        return pl.ds(order.index(d) * cap, cap)

    head = qg_hbm.shape[1]
    lane_count = 2 * head
    kv_index = lax.div(tp * heads, repeat)
    kv_lanes = pl.ds(pl.multiple_of(lax.div(kv_index, 2) * lane_count, lane_count), lane_count)
    ins = [
        pltpu.make_async_copy(src, dst, in_sem.at[i])
        for i, (src, dst) in enumerate((
            (route_hbm, route_ref), (logit_hbm, logit_ref), (x_hbm, x_ref), (pre_hbm, pre_ref),
            (k_hbm.at[:, kv_lanes], k_in), (v_hbm.at[:, kv_lanes], v_in), (turn_hbm, turn_ref), (kg_hbm, kg_ref),
            (q_hbm, q_in), (qg_hbm, qg_ref), (gain_hbm, gain_ref), (wout_hbm, wout_ref.at[:, cols_of(wout_hbm)]),
        ))
    ]
    for copy in ins:
        copy.start()
    loads = [
        pltpu.make_async_copy(src, dst, w_sem.at[i])
        for i, (src, dst) in enumerate(((wg_hbm, wg.at[:, cols_of(wg_hbm)]), (wu_hbm, wu.at[:, cols_of(wu_hbm)]), (wd_hbm, wd.at[:, cols_of(wd_hbm)])))
    ]
    for copy in loads:
        copy.start()
    barrier = pltpu.get_barrier_semaphore()
    for d in range(1, n_ep):
        pl.semaphore_signal(barrier, inc=1, device_id=(ep_at(d), tp), device_id_type=MESH)
    for d in range(1, ny):
        pl.semaphore_signal(barrier, inc=1, device_id=(ep, same_core(d)), device_id_type=MESH)
    pl.semaphore_signal(barrier, inc=1, device_id=(ep, partner), device_id_type=MESH)

    top, tokens = logit_ref.shape
    ins[0].wait()
    ins[1].wait()
    logits = logit_ref[...]
    power = jnp.exp(logits - jnp.max(logits, axis=0, keepdims=True))
    chance = power / jnp.sum(power, axis=0, keepdims=True)
    expert = lax.broadcasted_iota(jnp.int32, (n_ep, tokens), 0)
    named = jnp.zeros((n_ep, tokens), f32)
    share = jnp.zeros((n_ep, tokens), f32)
    for j in range(top):
        hit = route_ref[j : j + 1, :] == expert
        named = jnp.where(hit, 1.0, named)
        share = jnp.where(hit, chance[j : j + 1, :], share)
    above = lax.broadcasted_iota(jnp.int32, (tokens, tokens), 0) < lax.broadcasted_iota(
        jnp.int32, (tokens, tokens), 1
    )
    rank = jnp.dot(named, jnp.where(above, 1.0, 0.0), preferred_element_type=f32)
    rank = jnp.where(named > 0.0, rank, -1.0)
    place = lax.broadcasted_iota(jnp.int32, (cap, tokens), 0).astype(f32)
    for e in range(n_ep):
        there = rank[e : e + 1, :] == place
        placed_ref[e * cap : (e + 1) * cap, :] = jnp.where(there, 1.0, 0.0).astype(bf16)
        mixw_ref[e * cap : (e + 1) * cap, :] = jnp.where(there, share[e : e + 1, :], 0.0)

    ins[2].wait()
    ins[3].wait()
    x = x_ref[...].astype(f32)
    scale = lax.rsqrt(jnp.mean(x * x, axis=-1, keepdims=True) + EPSILON)
    mine = pl.ds(pl.multiple_of(tp * dq, dq), dq)
    normed = (x_ref[:, mine].astype(f32) * scale * pre_ref[:, mine]).astype(bf16)
    outgo_ref[...] = jnp.dot(placed_ref[...], normed, preferred_element_type=f32).astype(bf16)

    lane = lax.broadcasted_iota(jnp.int32, (GRID_W, lane_count), 1)
    first = lane < head
    ahead = lax.rem(lane, head // 2) < head // 4
    joined = lax.broadcasted_iota(jnp.int32, (lane_count, lane_count), 0) // head == (
        lax.broadcasted_iota(jnp.int32, (lane_count, lane_count), 1) // head
    )
    joined = jnp.where(joined, 1.0, 0.0).astype(bf16)
    blocks = rows_kv // GRID_W

    def turned(values, gain, b):
        square = values * values
        high = square.astype(bf16)
        low = (square - high.astype(f32)).astype(bf16)
        total = jnp.dot(high, joined, preferred_element_type=f32) + jnp.dot(
            low, joined, preferred_element_type=f32
        )
        values = values * lax.rsqrt(total * (1.0 / head) + EPSILON) * gain
        other = jnp.where(
            ahead,
            pltpu.roll(values, lane_count - head // 4, 1),
            pltpu.roll(values, head // 4, 1),
        )
        lines = turn_ref.shape[0] // 2 - GRID_W
        cos = turn_ref[pl.ds(ep * blocks + b, 1), :] + turn_ref[2 * lines : 2 * lines + GRID_W, :]
        sin = turn_ref[pl.ds(lines + ep * blocks + b, 1), :] + turn_ref[2 * lines + GRID_W :, :]
        return values * cos + other * sin

    odd = lax.rem(kv_index, 2)
    for copy in ins[4:8]:
        copy.wait()
    k_gain = jnp.concatenate([kg_ref[...], kg_ref[...]], axis=1)
    for b in range(blocks):
        at = slice(b * GRID_W, (b + 1) * GRID_W)
        keys = turned(k_in[at, :].astype(f32), k_gain, b)
        keys = jnp.where(odd == 1, pltpu.roll(keys, head, 1), keys)
        values = v_in[at, :].astype(f32)
        values = jnp.where(odd == 1, values, pltpu.roll(values, head, 1))
        kvbuf[ep, at, :] = jnp.where(first, keys, values).astype(bf16)
    with jax.named_scope("barrier"):
        pl.semaphore_wait(barrier, n_ep - 1 + ny - 1 + 1)

    disp = {
        d: remote(outgo_ref.at[slot_rows(flip(d))], arrived.at[held(d), lanes_of(tp)],
                  disp_s.at[d], disp_r.at[d], flip(d), tp)
        for d in range(1, n_ep)
    }

    def kv_line(b, target, sem):
        block = kvbuf.at[b * 2 + side]
        return remote(block, block, kz_s.at[sem], kz_r.at[b], target * 2 + side, tp)

    def kv_pass(b):
        block = kvbuf.at[b * 2 + side]
        return remote(block, block, kx_s.at[b], kx_r.at[b], mate, tp)

    has_next = col < nz - 1
    has_prev = col > 0

    kv_pass(col).start()
    for d in groups[0]:
        if d:
            disp[d].start()

    @pl.when(has_next)
    def _():
        kv_line(col, col + 1, col).start()

    @pl.when(has_prev)
    def _():
        kv_line(col, col - 1, nz).start()

    for d in groups[1]:
        disp[d].start()
    ins[8].wait()
    ins[9].wait()
    q_gain = jnp.concatenate([qg_ref[...], qg_ref[...]], axis=1)
    for g in range(max(1, heads // 2)):
        for b in range(blocks):
            at = slice(b * GRID_W, (b + 1) * GRID_W)
            if heads == 1:
                values = q_in[at, :].astype(f32)
                values = jnp.concatenate([values, jnp.zeros_like(values)], axis=1)
            else:
                values = q_in[at, g * lane_count : (g + 1) * lane_count].astype(f32)
            values = turned(values, q_gain, b) * (head ** (-0.5))
            for h in range(min(2, heads)):
                one = values if h == 0 else pltpu.roll(values, head, 1)
                one = jnp.where(first, one, 0.0).astype(bf16)
                for i in range(max(1, GRID_W // piece)):
                    size = min(piece, GRID_W)
                    token = b * GRID_W + i * size
                    row_at = (token // piece * heads + 2 * g + h) * piece + token % piece
                    q_ref[row_at : row_at + size, :] = one[i * size : (i + 1) * size, :]

    mine_rows = placed_ref[slot_rows(ep), :]
    for q in range(n_tp):
        at = slice(q * dq, (q + 1) * dq)
        full = (x_ref[:, at].astype(f32) * scale * pre_ref[:, at]).astype(bf16)
        arrived[held(0), at] = jnp.dot(mine_rows, full, preferred_element_type=f32).astype(bf16)

    q_rows = q_ref.shape[0]
    tile = min(512, heads * piece)

    def prepare(e, slot):
        keys = kvbuf[e]
        lanes = lax.broadcasted_iota(jnp.int32, keys.shape, 1)
        kt[slot] = keys.T
        vx[slot] = jnp.where(lanes < keys.shape[1] // 2, jnp.ones_like(keys), keys)

    def attend_rows(i, slot, fresh):
        for sub in range(2):
            at = pl.ds(pl.multiple_of(i * 2 * tile + sub * tile, tile), tile)
            scores = jnp.dot(q_ref[at, :], kt[slot], preferred_element_type=f32)
            weights = jnp.exp(scores).astype(bf16)
            term = jnp.dot(weights, vx[slot], preferred_element_type=f32)
            if fresh:
                acc[at, :] = term
            else:
                acc[at, :] += term

    def attend(e, fresh):
        prepare(e, 0)

        for i in range(q_rows // (2 * tile)):
            attend_rows(i, 0, fresh)

    shorter = jnp.minimum(col, nz - 1 - col)
    longer = jnp.where(col <= nz - 1 - col, 1, -1)

    def line_step(k):
        both = k < 2 * shorter
        way = jnp.where(both, 2 * lax.rem(k, 2) - 1, longer)
        far = jnp.where(both, lax.div(k, 2) + 1, k - shorter + 1)
        return col + way * far, col - way

    def line_one(k):
        b, target = line_step(k)
        wait("kv_line", kv_line(b, target, b))

        @pl.when(jnp.logical_and(target >= 0, target <= nz - 1))
        def _():
            kv_line(b, target, b).start()

        kv_pass(b).start()

    def line_take(k):
        both = k < 2 * shorter
        opening = jnp.logical_or(lax.rem(k, 2) == 0, jnp.logical_not(both))

        @pl.when(opening)
        def _():
            line_one(k)

        @pl.when(jnp.logical_and(opening, both))
        def _():
            line_one(k + 1)

    def line_end(early):
        middle = shorter > 0

        @pl.when(middle if early else jnp.logical_not(middle))
        def _():
            line_one(nz - 1 - 1)

    def line_block(k):
        return line_step(k)[0] * 2 + side

    def pass_block(k):
        b, _ = line_step(k)
        wait("kv_pass", kv_pass(b))
        return b * 2 + 1 - side

    def take(k, carry):
        line_take(k)
        attend(line_block(k), False)
        attend(pass_block(k), False)
        return carry

    def relay(d, dy):
        block = arrived.at[held(d), lanes_of(tp)]
        return remote(block, block, rel_s.at[d, dy], rel_r.at[d, dy], ep, same_core(dy))

    def foreign(c):
        count = len(groups[c]) - (1 if 0 in groups[c] else 0)
        return pl.ds(c * chunk, count * cap)

    def cross(c, dy):
        block = arrived.at[foreign(c), lanes_of(row_from(dy) * 2 + core)]
        if dy == 0:
            return remote(block, block, c0_s.at[c], c0_r.at[c], ep, partner)
        return remote(block, block, cy_s.at[c, dy], cy_r.at[c, dy], ep, partner)

    def relay_chunk(c):
        for d in groups[c]:
            if d:
                wait("disp", disp[d])
                for dy in range(1, ny):
                    relay(d, dy).start()
        cross(c, 0).start()

    def cross_chunk(c):
        for dy in range(1, ny):
            for d in groups[c]:
                if d:
                    wait("relay", relay(d, dy))
            cross(c, dy).start()

    ff = wg_hbm.shape[1]
    step = min(512, ff)

    def m1(c):
        return remote(pm.at[c, 1 - core], pm_in.at[c], m1_s.at[c], m1_r.at[c], ep, partner)

    def m2(c, s, dy):
        at = pl.ds(s * part, part)
        return remote(pm_red.at[c, lax.rem(row + dy, ny), at], pm_in2.at[c, row, at],
                      m2_s.at[c, s, dy], m2_r.at[c, s, dy], ep, same_core(dy))

    def chunk_rows(c):
        return slice(c * chunk, (c + 1) * chunk)

    def experts_up(c):
        for dy in range(ny):
            wait("cross", cross(c, dy))
        if c == 0:
            loads[0].wait()
            loads[1].wait()
        rows = chunk_rows(c)

        def gated(i, carry):
            at = pl.ds(pl.multiple_of(i * step, step), step)
            x = arrived[rows, : wg_hbm.shape[0]]
            gate = jnp.dot(x, wg[:, at], preferred_element_type=f32)
            up = jnp.dot(x, wu[:, at], preferred_element_type=f32)
            hidden[rows, at] = (gate / (1.0 + jnp.exp(-gate)) * up).astype(bf16)
            return carry

        lax.fori_loop(0, ff // step, gated, 0)

    def experts_down(c):
        rows = chunk_rows(c)
        if c == 0:
            loads[2].wait()

        def down_for(which):
            for y in range(ny):
                cols = pl.ds(pl.multiple_of((y * 2 + which) * dq, dq), dq)
                pm[c, which, y] = jnp.dot(
                    hidden[rows, :ff], wd[:, cols], preferred_element_type=f32
                ).astype(bf16)

        down_for(1 - core)
        m1(c).start()
        down_for(core)

    def reduce_cores(c):
        wait("m1", m1(c))
        for y in range(ny):
            pm_red[c, y] = (pm[c, core, y].astype(f32) + pm_in[c, y].astype(f32)).astype(bf16)
        for s in range(2):
            for dy in range(1, ny):
                m2(c, s, dy).start()

    def back(d):
        return remote(summed.at[held(d)], ret.at[slot_rows(ep)], ret_s.at[d], ret_r.at[d], flip(d), tp)

    def send_back(c):
        for s in range(2):
            for dy in range(1, ny):
                wait("m2", m2(c, s, dy))
            at = slice(s * part, (s + 1) * part)
            total = pm_red[c, row, at].astype(f32)
            for dy in range(1, ny):
                total = total + pm_in2[c, row_from(dy), at].astype(f32)
            total = total.astype(bf16)
            rows_at = c * chunk + s * part
            summed[rows_at : rows_at + part, :] = total
            for d in order[rows_at // cap : (rows_at + part) // cap]:
                if d:
                    back(d).start()
                else:
                    low = order.index(0) * cap - rows_at
                    ret[slot_rows(ep), :] = total[low : low + cap, :]

    tall = heads * piece
    half = acc.shape[1] // 2

    def finish(target):
        for slot in range(2):
            for i in range(2 * tall // (2 * tile)):
                attend_rows(target * (tall // tile) + i, slot, False)
        sides = []
        for c in range(2):
            which = core if c else 1 - core
            pieces = []
            for h in range(heads):
                at = pl.ds(pl.multiple_of((target * 2 + which) * tall + h * piece, piece), piece)
                sums = acc[at, :]
                pieces.append((sums[:, half:] / sums[:, :half]).astype(bf16))
            sides.append(pieces[0] if heads == 1 else jnp.concatenate(pieces, axis=1))
        both = jnp.concatenate(sides, axis=0)
        return jnp.dot(both, wout_ref[:, : wout_hbm.shape[1]], preferred_element_type=f32)

    def a1(d):
        return remote(pa.at[d], pa_in.at[d], a1_s.at[d], a1_r.at[d], ep, partner)

    def a2(d, s):
        at = pl.ds(s * (piece // 2), piece // 2)
        return remote(pa_red.at[d, at], pa_in2.at[d, at], a2_s.at[d, s], a2_r.at[d, s], ep, same_core(d))

    def finish_start(d):
        total = finish(lax.rem(row + d, ny)).astype(bf16)
        pa[d] = total[:piece]
        a1(d).start()
        pa_red[d] = total[piece:]

    def finish_end(d):
        wait("a1", a1(d))
        return pa_red[d].astype(f32) + pa_in[d].astype(f32)

    attend(ep, True)
    wait("kv_mate", kv_pass(col))
    attend(mate, False)
    relay_chunk(0)
    split = max(1, (nz - 1) // 2)
    brief = nz - 2 == split + 1
    line_take(0)
    attend(line_block(0), False)
    relay_chunk(1)
    cross_chunk(0)
    attend(pass_block(0), False)
    lax.fori_loop(1, split, take, 0)
    if brief:
        line_end(True)
    with jax.named_scope("up0"):
        experts_up(0)
    line_take(split)
    with jax.named_scope("down0"):
        experts_down(0)
    attend(line_block(split), False)
    reduce_cores(0)
    if brief:
        line_end(False)
    cross_chunk(1)
    attend(pass_block(split), False)
    lax.fori_loop(split + 1, nz - 2, take, 0)
    if not brief:
        line_take(nz - 2)
    prepare(line_block(nz - 2), 0)
    with jax.named_scope("up1"):
        experts_up(1)
    with jax.named_scope("down1"):
        experts_down(1)
    prepare(pass_block(nz - 2), 1)
    ins[10].wait()
    ins[11].wait()
    for d in range(1, ny):
        with jax.named_scope("finish"):
            finish_start(d)
    reduce_cores(1)
    send_back(0)
    for d in range(1, ny):
        pa_red[d] = finish_end(d).astype(bf16)
        for s in range(2):
            a2(d, s).start()
    with jax.named_scope("finish"):
        finish_start(0)
    send_back(1)
    pa_red[0] = finish_end(0).astype(bf16)
    for d in range(1, n_ep):
        wait("back", back(d))
    mixw = mixw_ref[...]
    high = mixw.astype(bf16)
    low = (mixw - high.astype(f32)).astype(bf16)
    over = (((0,), (0,)), ((), ()))
    moe_ref[...] = (
        lax.dot_general(high, ret[...], over, preferred_element_type=f32)
        + lax.dot_general(low, ret[...], over, preferred_element_type=f32)
    ).astype(bf16)
    for s in range(2):
        at = slice(s * (piece // 2), (s + 1) * (piece // 2))
        mixed = pa_red[0, at].astype(f32)
        for d in range(1, ny):
            wait("a2", a2(d, s))
            mixed = mixed + pa_in2[d, at].astype(f32)
        square = jnp.mean(mixed * mixed, axis=-1, keepdims=True)
        attn_ref[at, :] = (mixed * lax.rsqrt(square + EPSILON) * gain_ref[...]).astype(bf16)

    sent = [kv_pass(col)] + list(disp.values())
    sent += [relay(d, dy) for d in range(1, n_ep) for dy in range(1, ny)]
    sent += [cross(c, dy) for c in range(2) for dy in range(ny)]
    sent += [m1(c) for c in range(2)]
    sent += [m2(c, s, dy) for c in range(2) for s in range(2) for dy in range(1, ny)]
    sent += [back(d) for d in range(1, n_ep)]
    sent += [a1(d) for d in range(ny)] + [a2(d, s) for d in range(1, ny) for s in range(2)]
    for copy in sent:
        copy.wait_send()

    @pl.when(has_next)
    def _():
        kv_line(col, col + 1, col).wait_send()

    @pl.when(has_prev)
    def _():
        kv_line(col, col - 1, nz).wait_send()

    def kv_done(k, carry):
        b, target = line_step(k)

        @pl.when(jnp.logical_and(target >= 0, target <= nz - 1))
        def _():
            kv_line(b, target, b).wait_send()

        kv_pass(b).wait_send()
        return carry

    lax.fori_loop(0, nz - 1, kv_done, 0)


def per_device(
    n_ep, n_tp,
    q_in, k_in, v_in, q_gain, k_gain, w_out, post_gain,
    moe_in, routes, route_logits, pre_gain, w_gate, w_up, w_down,
):
    bf16 = jnp.bfloat16
    head = q_gain.shape[0]
    rows = q_in.shape[0]
    heads = q_in.shape[1] // head
    kv_count = k_in.shape[1] // head
    repeat = heads * n_tp // kv_count
    ny = n_tp // 2
    nz = n_ep // 2
    turns = turn_tables(n_ep * rows, GRID_W, head // 4)

    tokens, top = routes.shape
    width = moe_in.shape[1]
    dq = width // n_tp
    need = max(2, 3 * top * tokens // (2 * n_ep))
    cap = -(-need // 16) * 16
    slots = n_ep * cap

    piece = rows // n_tp
    ff = w_gate.shape[2]
    dma = pltpu.SemaphoreType.DMA
    vmem = pl.BlockSpec(memory_space=pltpu.VMEM)
    hbm = pl.BlockSpec(memory_space=pl.ANY)
    return pl.pallas_call(
        functools.partial(kernel, (n_ep, n_tp, heads, cap, repeat)),
        out_shape=(
            pltpu.VMEM((piece, width), bf16),
            pltpu.VMEM((tokens, dq), bf16),
        ),
        in_specs=[hbm] * 15,
        out_specs=(vmem, vmem),
        scratch_shapes=[
            pltpu.VMEM((top, tokens), jnp.int32),
            pltpu.VMEM((top, tokens), jnp.float32),
            pltpu.VMEM((1, width), jnp.float32),
            pltpu.VMEM((1, width), jnp.float32),
            pltpu.VMEM((1, head), jnp.float32),
            pltpu.VMEM((1, head), jnp.float32),
            pltpu.VMEM(turns.shape, jnp.float32),
            pltpu.VMEM((rows, heads * head), bf16),
            pltpu.VMEM((rows, 2 * head), bf16),
            pltpu.VMEM((rows, 2 * head), bf16),
            pltpu.VMEM((tokens, width), bf16),
            pltpu.VMEM((heads * head, width + SKEW), bf16),
            pltpu.VMEM((heads * rows, 2 * head), bf16),
            pltpu.VMEM((slots, tokens), bf16),
            pltpu.VMEM((slots, dq), bf16),
            pltpu.VMEM((slots, tokens), jnp.float32),
            pltpu.VMEM((width, ff + SKEW), bf16),
            pltpu.VMEM((width, ff + SKEW), bf16),
            pltpu.VMEM((ff, width + SKEW), bf16),
            pltpu.VMEM((n_ep, rows, 2 * head), bf16),
            pltpu.VMEM((2, rows, 2 * head), bf16),
            pltpu.VMEM((2, 2 * head, rows), bf16),
            pltpu.VMEM((heads * rows, 2 * head), jnp.float32),
            pltpu.VMEM((slots, width + SKEW), bf16),
            pltpu.VMEM((slots, ff + SKEW), bf16),
            pltpu.VMEM((ny, piece, width), bf16),
            pltpu.VMEM((ny, piece, width), bf16),
            pltpu.VMEM((ny, piece, width), bf16),
            pltpu.VMEM((ny, piece, width), bf16),
            pltpu.VMEM((2, 2, ny, slots // 2, dq), bf16),
            pltpu.VMEM((2, ny, slots // 2, dq), bf16),
            pltpu.VMEM((2, ny, slots // 2, dq), bf16),
            pltpu.VMEM((2, ny, slots // 2, dq), bf16),
            pltpu.VMEM((slots, dq), bf16),
            pltpu.VMEM((slots, dq), bf16),
            dma((12,)), dma((3,)),
            dma((nz + 1,)), dma((nz,)), dma((nz,)), dma((nz,)),
            dma((n_ep,)), dma((n_ep,)), dma((n_ep, ny)), dma((n_ep, ny)),
            dma((2,)), dma((2,)), dma((2, ny)), dma((2, ny)),
            dma((ny,)), dma((ny,)), dma((ny, 2)), dma((ny, 2)),
            dma((2,)), dma((2,)), dma((2, 2, ny)), dma((2, 2, ny)),
            dma((n_ep,)), dma((n_ep,)),
        ],
        compiler_params=pltpu.CompilerParams(
            collective_id=0, has_side_effects=True, vmem_limit_bytes=VMEM_LIMIT
        ),
    )(
        routes.T, route_logits.T, pre_gain[None, :], post_gain[None, :], q_gain[None, :], k_gain[None, :], turns,
        q_in, k_in, v_in, moe_in, w_out, w_gate[0], w_up[0], w_down[0],
    )


def solution(mesh):
    return jax.shard_map(
        functools.partial(per_device, mesh.shape["ep"], mesh.shape["tp"]),
        mesh=mesh,
        in_specs=(
            P("ep", "tp"),
            P("ep", None),
            P("ep", None),
            P(),
            P(),
            P("tp", None),
            P(),
            P("ep", None),
            P("ep", None),
            P("ep", None),
            P(),
            P("ep", None, "tp"),
            P("ep", None, "tp"),
            P("ep", "tp", None),
        ),
        out_specs=(P(("ep", "tp"), None), P("ep", "tp")),
        check_vma=False,
    )
```

```python
import functools

import jax
import jax.numpy as jnp
import numpy as np
from jax import lax
from jax.experimental import pallas as pl
from jax.experimental.pallas import tpu as pltpu
from jax.sharding import PartitionSpec as P

GRID_W = 128
EPSILON = 1e-06
ROPE_BASE = 10000.0
MESH = pl.DeviceIdType.MESH
SKEW = 128
VMEM_LIMIT = 60 * 1024 * 1024


def turn_tables(positions, rows_of_grid, quarter):
    inverse = ROPE_BASE ** (-np.arange(quarter, dtype=np.float32) / np.float32(quarter))
    inverse = inverse.astype(np.float32)

    def table(count, first_half):
        angles = (np.arange(count, dtype=np.float32)[:, None] * inverse[None, :]).astype(np.float64)
        cos, sin = np.cos(angles), np.sin(angles)
        none = np.zeros_like(cos)
        cos = np.concatenate([cos, cos, none, none] if first_half else [none, none, cos, cos], axis=1)
        sin = np.concatenate([-sin, sin, none, none] if first_half else [none, none, -sin, sin], axis=1)
        return np.concatenate([cos, cos], axis=1), np.concatenate([sin, sin], axis=1)

    grid_rows = positions // rows_of_grid
    by_row = table(grid_rows, True)
    by_col = table(rows_of_grid, False)
    return jnp.asarray(np.concatenate(by_row + by_col), jnp.float32)


def kernel(
    dims,
    route_hbm, logit_hbm, pre_hbm, gain_hbm, qg_hbm, kg_hbm, turn_hbm,
    q_hbm, k_hbm, v_hbm, x_hbm, wout_hbm, wg_hbm, wu_hbm, wd_hbm,
    attn_ref, moe_ref,
    route_ref, logit_ref, pre_ref, gain_ref, qg_ref, kg_ref, turn_ref,
    q_in, k_in, v_in, x_ref, wout_ref, q_ref, placed_ref,
    outgo_ref, mixw_ref, wg, wu, wd, kvbuf, vx, kt, acc, arrived, hidden,
    wall, ho_out, ho_in, whole, pa, pa_in, pa_red, pa_in2, pm, pm_in, pm_red, pm_in2, summed, ret,
    in_sem, w_sem, kz_s, kz_r, kx_s, kx_r, disp_s, disp_r, rel_s, rel_r, c0_s, c0_r, cy_s, cy_r,
    w0_s, w0_r, wy_s, wy_r, wc_s, wc_r, ho_s, ho_r, a1_s, a1_r, a2_s, a2_r, m1_s, m1_r, m2_s, m2_r, ret_s, ret_r,
):
    n_ep, n_tp, heads, cap, repeat = dims
    ny = n_tp // 2
    nz = n_ep // 2
    ep = lax.axis_index("ep")
    tp = lax.axis_index("tp")
    core = lax.rem(tp, 2)
    row = lax.div(tp, 2)
    partner = row * 2 + 1 - core
    side = lax.rem(ep, 2)
    col = lax.div(ep, 2)
    mate = col * 2 + 1 - side
    rows_kv = k_in.shape[0]
    dq = outgo_ref.shape[1]
    slots = outgo_ref.shape[0]
    piece = attn_ref.shape[0]
    bf16, f32 = jnp.bfloat16, jnp.float32

    def remote(src, dst, ss, rs, e, t):
        return pltpu.make_async_remote_copy(
            src_ref=src, dst_ref=dst, send_sem=ss, recv_sem=rs,
            device_id=(e, t), device_id_type=MESH,
        )

    def wait(name, copy):
        with jax.named_scope(name):
            copy.wait_recv()

    def ep_at(d):
        return lax.rem(ep + d, n_ep)

    def flip(d):
        other = ep
        for bit in range(n_ep.bit_length() - 1):
            if (d >> bit) % 2:
                other = other + (1 << bit) * (1 - 2 * lax.rem(lax.div(ep, 1 << bit), 2))
        return other

    def same_core(d):
        return lax.rem(row + d, ny) * 2 + core

    def row_from(d):
        return lax.rem(row - d + ny, ny)

    def slot_rows(e):
        return pl.ds(pl.multiple_of(e * cap, cap), cap)

    def cols_of(ref):
        return pl.ds(0, ref.shape[1])

    narrow = pa.shape[2]
    wide = wout_hbm.shape[1] - narrow
    dims_here = wout_hbm.shape[0]
    parts = wy_s.shape[1]
    strip = dims_here // parts
    starts = (parts * 5 // 8, parts * 7 // 8)

    def wall_rows(t, i, count):
        first_row = pl.multiple_of(t * dims_here + i * strip, strip)
        return wall.at[pl.ds(first_row, count * strip), pl.ds(0, wide)]

    def w_partner():
        block = wall_rows(tp, 0, parts)
        return remote(block, block, w0_s.at[0], w0_r.at[0], ep, partner)

    def w_row(dy, i):
        block = wall_rows(tp, i, 1)
        return remote(block, block, wy_s.at[dy, i], wy_r.at[dy, i], ep, same_core(dy))

    def w_cross(dy):
        block = wall_rows(row_from(dy) * 2 + core, 0, parts)
        return remote(block, block, wc_s.at[dy], wc_r.at[dy], ep, partner)

    def w_send(i):
        for dy in range(1, ny):
            w_row(dy, i).start()

    def lanes_of(t):
        return pl.ds(pl.multiple_of(t * dq, dq), dq)

    quarter = n_ep // 4
    near = list(range(quarter - 1, -1, -1))
    groups = [
        list(range(2 * quarter, 3 * quarter)) + near,
        list(range(3 * quarter, 4 * quarter)) + list(range(quarter, 2 * quarter)),
    ]
    order = groups[0] + groups[1]
    chunk = slots // 2
    part = chunk // 2

    def held(d):
        return pl.ds(order.index(d) * cap, cap)

    head = qg_hbm.shape[1]
    lane_count = 2 * head
    kv_index = lax.div(tp * heads, repeat)
    kv_lanes = pl.ds(pl.multiple_of(lax.div(kv_index, 2) * lane_count, lane_count), lane_count)
    ins = [
        pltpu.make_async_copy(src, dst, in_sem.at[i])
        for i, (src, dst) in enumerate((
            (route_hbm, route_ref), (logit_hbm, logit_ref), (x_hbm, x_ref), (pre_hbm, pre_ref),
            (k_hbm.at[:, kv_lanes], k_in), (v_hbm.at[:, kv_lanes], v_in), (turn_hbm, turn_ref), (kg_hbm, kg_ref),
            (q_hbm, q_in), (qg_hbm, qg_ref), (gain_hbm, gain_ref), (wout_hbm.at[:, pl.ds(0, narrow)], wout_ref.at[:, pl.ds(0, narrow)]),
            (wout_hbm.at[:, pl.ds(narrow, wide)], wall_rows(tp, 0, parts)),
        ))
    ]
    for copy in ins:
        copy.start()
    loads = [
        pltpu.make_async_copy(src, dst, w_sem.at[i])
        for i, (src, dst) in enumerate(((wg_hbm, wg.at[:, cols_of(wg_hbm)]), (wu_hbm, wu.at[:, cols_of(wu_hbm)]), (wd_hbm, wd.at[:, cols_of(wd_hbm)])))
    ]
    for copy in loads:
        copy.start()
    barrier = pltpu.get_barrier_semaphore()
    for d in range(1, n_ep):
        pl.semaphore_signal(barrier, inc=1, device_id=(ep_at(d), tp), device_id_type=MESH)
    for d in range(1, ny):
        pl.semaphore_signal(barrier, inc=1, device_id=(ep, same_core(d)), device_id_type=MESH)
    pl.semaphore_signal(barrier, inc=1, device_id=(ep, partner), device_id_type=MESH)

    top, tokens = logit_ref.shape
    ins[0].wait()
    ins[1].wait()
    logits = logit_ref[...]
    power = jnp.exp(logits - jnp.max(logits, axis=0, keepdims=True))
    chance = power / jnp.sum(power, axis=0, keepdims=True)
    expert = lax.broadcasted_iota(jnp.int32, (n_ep, tokens), 0)
    named = jnp.zeros((n_ep, tokens), f32)
    share = jnp.zeros((n_ep, tokens), f32)
    for j in range(top):
        hit = route_ref[j : j + 1, :] == expert
        named = jnp.where(hit, 1.0, named)
        share = jnp.where(hit, chance[j : j + 1, :], share)
    above = lax.broadcasted_iota(jnp.int32, (tokens, tokens), 0) < lax.broadcasted_iota(
        jnp.int32, (tokens, tokens), 1
    )
    rank = jnp.dot(named, jnp.where(above, 1.0, 0.0), preferred_element_type=f32)
    rank = jnp.where(named > 0.0, rank, -1.0)
    place = lax.broadcasted_iota(jnp.int32, (cap, tokens), 0).astype(f32)
    for e in range(n_ep):
        there = rank[e : e + 1, :] == place
        placed_ref[e * cap : (e + 1) * cap, :] = jnp.where(there, 1.0, 0.0).astype(bf16)
        mixw_ref[e * cap : (e + 1) * cap, :] = jnp.where(there, share[e : e + 1, :], 0.0)

    ins[2].wait()
    ins[3].wait()
    x = x_ref[...].astype(f32)
    scale = lax.rsqrt(jnp.mean(x * x, axis=-1, keepdims=True) + EPSILON)
    mine = pl.ds(pl.multiple_of(tp * dq, dq), dq)
    normed = (x_ref[:, mine].astype(f32) * scale * pre_ref[:, mine]).astype(bf16)
    outgo_ref[...] = jnp.dot(placed_ref[...], normed, preferred_element_type=f32).astype(bf16)

    lane = lax.broadcasted_iota(jnp.int32, (GRID_W, lane_count), 1)
    first = lane < head
    ahead = lax.rem(lane, head // 2) < head // 4
    joined = lax.broadcasted_iota(jnp.int32, (lane_count, lane_count), 0) // head == (
        lax.broadcasted_iota(jnp.int32, (lane_count, lane_count), 1) // head
    )
    joined = jnp.where(joined, 1.0, 0.0).astype(bf16)
    blocks = rows_kv // GRID_W

    def turned(values, gain, b):
        square = values * values
        high = square.astype(bf16)
        low = (square - high.astype(f32)).astype(bf16)
        total = jnp.dot(high, joined, preferred_element_type=f32) + jnp.dot(
            low, joined, preferred_element_type=f32
        )
        values = values * lax.rsqrt(total * (1.0 / head) + EPSILON) * gain
        other = jnp.where(
            ahead,
            pltpu.roll(values, lane_count - head // 4, 1),
            pltpu.roll(values, head // 4, 1),
        )
        lines = turn_ref.shape[0] // 2 - GRID_W
        cos = turn_ref[pl.ds(ep * blocks + b, 1), :] + turn_ref[2 * lines : 2 * lines + GRID_W, :]
        sin = turn_ref[pl.ds(lines + ep * blocks + b, 1), :] + turn_ref[2 * lines + GRID_W :, :]
        return values * cos + other * sin

    odd = lax.rem(kv_index, 2)
    for copy in ins[4:8]:
        copy.wait()
    k_gain = jnp.concatenate([kg_ref[...], kg_ref[...]], axis=1)
    for b in range(blocks):
        at = slice(b * GRID_W, (b + 1) * GRID_W)
        keys = turned(k_in[at, :].astype(f32), k_gain, b)
        keys = jnp.where(odd == 1, pltpu.roll(keys, head, 1), keys)
        values = v_in[at, :].astype(f32)
        values = jnp.where(odd == 1, values, pltpu.roll(values, head, 1))
        kvbuf[ep, at, :] = jnp.where(first, keys, values).astype(bf16)
    with jax.named_scope("barrier"):
        pl.semaphore_wait(barrier, n_ep - 1 + ny - 1 + 1)

    disp = {
        d: remote(outgo_ref.at[slot_rows(flip(d))], arrived.at[held(d), lanes_of(tp)],
                  disp_s.at[d], disp_r.at[d], flip(d), tp)
        for d in range(1, n_ep)
    }

    def kv_line(b, target, sem):
        block = kvbuf.at[b * 2 + side]
        return remote(block, block, kz_s.at[sem], kz_r.at[b], target * 2 + side, tp)

    def kv_pass(b):
        block = kvbuf.at[b * 2 + side]
        return remote(block, block, kx_s.at[b], kx_r.at[b], mate, tp)

    has_next = col < nz - 1
    has_prev = col > 0

    for d in groups[0]:
        if d:
            disp[d].start()
    kv_pass(col).start()

    @pl.when(has_next)
    def _():
        kv_line(col, col + 1, col).start()

    @pl.when(has_prev)
    def _():
        kv_line(col, col - 1, nz).start()

    for d in groups[1]:
        disp[d].start()
    ins[12].wait()
    for i in range(starts[0]):
        w_send(i)
    w_partner().start()
    ins[8].wait()
    ins[9].wait()
    q_gain = jnp.concatenate([qg_ref[...], qg_ref[...]], axis=1)
    for g in range(max(1, heads // 2)):
        for b in range(blocks):
            at = slice(b * GRID_W, (b + 1) * GRID_W)
            if heads == 1:
                values = q_in[at, :].astype(f32)
                values = jnp.concatenate([values, jnp.zeros_like(values)], axis=1)
            else:
                values = q_in[at, g * lane_count : (g + 1) * lane_count].astype(f32)
            values = turned(values, q_gain, b) * (head ** (-0.5))
            for h in range(min(2, heads)):
                one = values if h == 0 else pltpu.roll(values, head, 1)
                one = jnp.where(first, one, 0.0).astype(bf16)
                for i in range(max(1, GRID_W // piece)):
                    size = min(piece, GRID_W)
                    token = b * GRID_W + i * size
                    row_at = (token // piece * heads + 2 * g + h) * piece + token % piece
                    q_ref[row_at : row_at + size, :] = one[i * size : (i + 1) * size, :]

    mine_rows = placed_ref[slot_rows(ep), :]
    for q in range(n_tp):
        at = slice(q * dq, (q + 1) * dq)
        full = (x_ref[:, at].astype(f32) * scale * pre_ref[:, at]).astype(bf16)
        arrived[held(0), at] = jnp.dot(mine_rows, full, preferred_element_type=f32).astype(bf16)

    q_rows = q_ref.shape[0]
    tile = min(512, heads * piece)

    def prepare(e, slot):
        keys = kvbuf[e]
        lanes = lax.broadcasted_iota(jnp.int32, keys.shape, 1)
        kt[slot] = keys.T
        vx[slot] = jnp.where(lanes < keys.shape[1] // 2, jnp.ones_like(keys), keys)

    def attend_rows(i, slot, fresh):
        for sub in range(2):
            at = pl.ds(pl.multiple_of(i * 2 * tile + sub * tile, tile), tile)
            scores = jnp.dot(q_ref[at, :], kt[slot], preferred_element_type=f32)
            weights = jnp.exp(scores).astype(bf16)
            term = jnp.dot(weights, vx[slot], preferred_element_type=f32)
            if fresh:
                acc[at, :] = term
            else:
                acc[at, :] += term

    def attend(e, fresh):
        prepare(e, 0)

        for i in range(q_rows // (2 * tile)):
            attend_rows(i, 0, fresh)

    shorter = jnp.minimum(col, nz - 1 - col)
    longer = jnp.where(col <= nz - 1 - col, 1, -1)

    def line_step(k):
        both = k < 2 * shorter
        way = jnp.where(both, 2 * lax.rem(k, 2) - 1, longer)
        far = jnp.where(both, lax.div(k, 2) + 1, k - shorter + 1)
        return col + way * far, col - way

    def line_one(k):
        b, target = line_step(k)
        wait("kv_line", kv_line(b, target, b))

        @pl.when(jnp.logical_and(target >= 0, target <= nz - 1))
        def _():
            kv_line(b, target, b).start()

        kv_pass(b).start()

    def line_take(k):
        both = k < 2 * shorter
        opening = jnp.logical_or(lax.rem(k, 2) == 0, jnp.logical_not(both))

        @pl.when(opening)
        def _():
            line_one(k)

        @pl.when(jnp.logical_and(opening, both))
        def _():
            line_one(k + 1)

    def line_end(early):
        middle = shorter > 0

        @pl.when(middle if early else jnp.logical_not(middle))
        def _():
            line_one(nz - 1 - 1)

    def line_block(k):
        return line_step(k)[0] * 2 + side

    def pass_block(k):
        b, _ = line_step(k)
        wait("kv_pass", kv_pass(b))
        return b * 2 + 1 - side

    def take(k, carry):
        line_take(k)
        attend(line_block(k), False)
        attend(pass_block(k), False)
        return carry

    def relay(d, dy):
        block = arrived.at[held(d), lanes_of(tp)]
        return remote(block, block, rel_s.at[d, dy], rel_r.at[d, dy], ep, same_core(dy))

    def foreign(c):
        count = len(groups[c]) - (1 if 0 in groups[c] else 0)
        return pl.ds(c * chunk, count * cap)

    def cross(c, dy):
        block = arrived.at[foreign(c), lanes_of(row_from(dy) * 2 + core)]
        if dy == 0:
            return remote(block, block, c0_s.at[c], c0_r.at[c], ep, partner)
        return remote(block, block, cy_s.at[c, dy], cy_r.at[c, dy], ep, partner)

    def relay_chunk(c):
        for d in groups[c]:
            if d:
                wait("disp", disp[d])
                for dy in range(1, ny):
                    relay(d, dy).start()
        cross(c, 0).start()

    def cross_chunk(c):
        for dy in range(1, ny):
            for d in groups[c]:
                if d:
                    wait("relay", relay(d, dy))
            cross(c, dy).start()

    ff = wg_hbm.shape[1]
    step = min(512, ff)

    def m1(c):
        return remote(pm.at[c, 1 - core], pm_in.at[c], m1_s.at[c], m1_r.at[c], ep, partner)

    def m2(c, s, dy):
        at = pl.ds(s * part, part)
        return remote(pm_red.at[c, lax.rem(row + dy, ny), at], pm_in2.at[c, row, at],
                      m2_s.at[c, s, dy], m2_r.at[c, s, dy], ep, same_core(dy))

    def chunk_rows(c):
        return slice(c * chunk, (c + 1) * chunk)

    def experts_up(c):
        for dy in range(ny):
            wait("cross", cross(c, dy))
        if c == 0:
            loads[0].wait()
            loads[1].wait()
        rows = chunk_rows(c)

        def gated(i, carry):
            at = pl.ds(pl.multiple_of(i * step, step), step)
            x = arrived[rows, : wg_hbm.shape[0]]
            gate = jnp.dot(x, wg[:, at], preferred_element_type=f32)
            up = jnp.dot(x, wu[:, at], preferred_element_type=f32)
            hidden[rows, at] = (gate / (1.0 + jnp.exp(-gate)) * up).astype(bf16)
            return carry

        lax.fori_loop(0, ff // step, gated, 0)

    def experts_down(c):
        rows = chunk_rows(c)
        if c == 0:
            loads[2].wait()

        def down_for(which):
            for y in range(ny):
                cols = pl.ds(pl.multiple_of((y * 2 + which) * dq, dq), dq)
                pm[c, which, y] = jnp.dot(
                    hidden[rows, :ff], wd[:, cols], preferred_element_type=f32
                ).astype(bf16)

        down_for(1 - core)
        m1(c).start()
        down_for(core)

    def reduce_cores(c):
        wait("m1", m1(c))
        for y in range(ny):
            pm_red[c, y] = (pm[c, core, y].astype(f32) + pm_in[c, y].astype(f32)).astype(bf16)
        for s in range(2):
            for dy in range(1, ny):
                m2(c, s, dy).start()

    def back(d):
        return remote(summed.at[held(d)], ret.at[slot_rows(ep)], ret_s.at[d], ret_r.at[d], flip(d), tp)

    def send_back(c):
        for s in range(2):
            for dy in range(1, ny):
                wait("m2", m2(c, s, dy))
            at = slice(s * part, (s + 1) * part)
            total = pm_red[c, row, at].astype(f32)
            for dy in range(1, ny):
                total = total + pm_in2[c, row_from(dy), at].astype(f32)
            total = total.astype(bf16)
            rows_at = c * chunk + s * part
            summed[rows_at : rows_at + part, :] = total
            for d in order[rows_at // cap : (rows_at + part) // cap]:
                if d:
                    back(d).start()
                else:
                    low = order.index(0) * cap - rows_at
                    ret[slot_rows(ep), :] = total[low : low + cap, :]

    tall = heads * piece
    half = acc.shape[1] // 2

    def finish(target):
        for slot in range(2):
            for i in range(2 * tall // (2 * tile)):
                attend_rows(target * (tall // tile) + i, slot, False)
        sides = []
        for c in range(2):
            which = core if c else 1 - core
            pieces = []
            for h in range(heads):
                at = pl.ds(pl.multiple_of((target * 2 + which) * tall + h * piece, piece), piece)
                sums = acc[at, :]
                pieces.append((sums[:, half:] / sums[:, :half]).astype(bf16))
            sides.append(pieces[0] if heads == 1 else jnp.concatenate(pieces, axis=1))
        return sides

    def a1(d):
        return remote(pa.at[d], pa_in.at[d], a1_s.at[d], a1_r.at[d], ep, partner)

    def a2(d, s):
        at = pl.ds(s * (piece // 2), piece // 2)
        return remote(pa_red.at[d, at], pa_in2.at[d, at], a2_s.at[d, s], a2_r.at[d, s], ep, same_core(d))

    def ho(d, c):
        target = lax.rem(row + d, ny) * 2 + (core if c else 1 - core)
        return remote(ho_out.at[2 * d + c], ho_in.at[tp], ho_s.at[2 * d + c], ho_r.at[2 * d + c], ep, target)

    def finish_start(d):
        sides = finish(lax.rem(row + d, ny))
        for c in range(2):
            if d == 0 and c == 1:
                ho_in[tp] = sides[1]
            else:
                ho_out[2 * d + c] = sides[c]
                ho(d, c).start()
        both = jnp.concatenate(sides, axis=0)
        total = jnp.dot(both, wout_ref[:, :narrow], preferred_element_type=f32).astype(bf16)
        pa[d] = total[:piece]
        a1(d).start()
        pa_red[d] = total[piece:]

    def finish_end(d):
        wait("a1", a1(d))
        return pa_red[d].astype(f32) + pa_in[d].astype(f32)

    attend(ep, True)
    relay_chunk(0)
    wait("kv_mate", kv_pass(col))
    attend(mate, False)
    split = max(1, (nz - 1) // 2)
    brief = nz - 2 == split + 1
    line_take(0)
    attend(line_block(0), False)
    relay_chunk(1)
    for i in range(*starts):
        w_send(i)
    cross_chunk(0)
    attend(pass_block(0), False)
    lax.fori_loop(1, split, take, 0)
    if brief:
        line_end(True)
    with jax.named_scope("up0"):
        experts_up(0)
    line_take(split)
    with jax.named_scope("down0"):
        experts_down(0)
    cross_chunk(1)
    attend(line_block(split), False)
    reduce_cores(0)
    for i in range(starts[1], parts):
        w_send(i)
    with jax.named_scope("up1"):
        experts_up(1)
    if brief:
        line_end(False)
    with jax.named_scope("down1"):
        experts_down(1)
    attend(pass_block(split), False)
    lax.fori_loop(split + 1, nz - 2, take, 0)
    if not brief:
        line_take(nz - 2)
    reduce_cores(1)
    send_back(0)
    prepare(line_block(nz - 2), 0)
    prepare(pass_block(nz - 2), 1)
    ins[10].wait()
    ins[11].wait()
    for d in range(1, ny):
        with jax.named_scope("finish"):
            finish_start(d)
    for dy in range(1, ny):
        for i in range(parts):
            wait("w_row", w_row(dy, i))
        w_cross(dy).start()
    for d in range(1, ny):
        pa_red[d] = finish_end(d).astype(bf16)
        for s in range(2):
            a2(d, s).start()
    with jax.named_scope("finish"):
        finish_start(0)
    send_back(1)
    pa_red[0] = finish_end(0).astype(bf16)
    wait("w_partner", w_partner())
    for dy in range(1, ny):
        wait("w_cross", w_cross(dy))
    for d in range(ny):
        for c in range(2):
            if d or c == 0:
                wait("ho", ho(d, c))
    gathered = jnp.concatenate([ho_in[t] for t in range(n_tp)], axis=1)
    whole[...] = jnp.dot(gathered, wall[:, :wide], preferred_element_type=f32)
    for s in range(2):
        at = slice(s * (piece // 2), (s + 1) * (piece // 2))
        mixed = pa_red[0, at].astype(f32)
        for d in range(1, ny):
            wait("a2", a2(d, s))
            mixed = mixed + pa_in2[d, at].astype(f32)
        rest = whole[at, :]
        square = jnp.sum(mixed * mixed, axis=-1, keepdims=True) + jnp.sum(rest * rest, axis=-1, keepdims=True)
        scale = lax.rsqrt(square * (1.0 / (narrow + wide)) + EPSILON)
        attn_ref[at, :narrow] = (mixed * scale * gain_ref[:, :narrow]).astype(bf16)
        attn_ref[at, narrow:] = (rest * scale * gain_ref[:, narrow:]).astype(bf16)

    for d in range(1, n_ep):
        wait("back", back(d))
    mixw = mixw_ref[...]
    high = mixw.astype(bf16)
    low = (mixw - high.astype(f32)).astype(bf16)
    over = (((0,), (0,)), ((), ()))
    moe_ref[...] = (
        lax.dot_general(high, ret[...], over, preferred_element_type=f32)
        + lax.dot_general(low, ret[...], over, preferred_element_type=f32)
    ).astype(bf16)
    sent = [kv_pass(col)] + list(disp.values())
    sent += [relay(d, dy) for d in range(1, n_ep) for dy in range(1, ny)]
    sent += [cross(c, dy) for c in range(2) for dy in range(ny)]
    sent += [m1(c) for c in range(2)]
    sent += [m2(c, s, dy) for c in range(2) for s in range(2) for dy in range(1, ny)]
    sent += [back(d) for d in range(1, n_ep)]
    sent += [w_partner()] + [w_row(dy, i) for dy in range(1, ny) for i in range(parts)]
    sent += [w_cross(dy) for dy in range(1, ny)]
    sent += [ho(d, c) for d in range(ny) for c in range(2) if d or c == 0]
    sent += [a1(d) for d in range(ny)] + [a2(d, s) for d in range(1, ny) for s in range(2)]
    for copy in sent:
        copy.wait_send()

    @pl.when(has_next)
    def _():
        kv_line(col, col + 1, col).wait_send()

    @pl.when(has_prev)
    def _():
        kv_line(col, col - 1, nz).wait_send()

    def kv_done(k, carry):
        b, target = line_step(k)

        @pl.when(jnp.logical_and(target >= 0, target <= nz - 1))
        def _():
            kv_line(b, target, b).wait_send()

        kv_pass(b).wait_send()
        return carry

    lax.fori_loop(0, nz - 1, kv_done, 0)


def per_device(
    n_ep, n_tp,
    q_in, k_in, v_in, q_gain, k_gain, w_out, post_gain,
    moe_in, routes, route_logits, pre_gain, w_gate, w_up, w_down,
):
    bf16 = jnp.bfloat16
    head = q_gain.shape[0]
    rows = q_in.shape[0]
    heads = q_in.shape[1] // head
    kv_count = k_in.shape[1] // head
    repeat = heads * n_tp // kv_count
    ny = n_tp // 2
    nz = n_ep // 2
    turns = turn_tables(n_ep * rows, GRID_W, head // 4)

    tokens, top = routes.shape
    width = moe_in.shape[1]
    dq = width // n_tp
    need = max(2, 3 * top * tokens // (2 * n_ep))
    cap = -(-need // 16) * 16
    slots = n_ep * cap

    piece = rows // n_tp
    ff = w_gate.shape[2]
    narrow = width // 2
    strips = min(8, heads * head // 16)
    dma = pltpu.SemaphoreType.DMA
    vmem = pl.BlockSpec(memory_space=pltpu.VMEM)
    hbm = pl.BlockSpec(memory_space=pl.ANY)
    return pl.pallas_call(
        functools.partial(kernel, (n_ep, n_tp, heads, cap, repeat)),
        out_shape=(
            pltpu.VMEM((piece, width), bf16),
            pltpu.VMEM((tokens, dq), bf16),
        ),
        in_specs=[hbm] * 15,
        out_specs=(vmem, vmem),
        scratch_shapes=[
            pltpu.VMEM((top, tokens), jnp.int32),
            pltpu.VMEM((top, tokens), jnp.float32),
            pltpu.VMEM((1, width), jnp.float32),
            pltpu.VMEM((1, width), jnp.float32),
            pltpu.VMEM((1, head), jnp.float32),
            pltpu.VMEM((1, head), jnp.float32),
            pltpu.VMEM(turns.shape, jnp.float32),
            pltpu.VMEM((rows, heads * head), bf16),
            pltpu.VMEM((rows, 2 * head), bf16),
            pltpu.VMEM((rows, 2 * head), bf16),
            pltpu.VMEM((tokens, width), bf16),
            pltpu.VMEM((heads * head, narrow + SKEW), bf16),
            pltpu.VMEM((heads * rows, 2 * head), bf16),
            pltpu.VMEM((slots, tokens), bf16),
            pltpu.VMEM((slots, dq), bf16),
            pltpu.VMEM((slots, tokens), jnp.float32),
            pltpu.VMEM((width, ff + SKEW), bf16),
            pltpu.VMEM((width, ff + SKEW), bf16),
            pltpu.VMEM((ff, width + SKEW), bf16),
            pltpu.VMEM((n_ep, rows, 2 * head), bf16),
            pltpu.VMEM((2, rows, 2 * head), bf16),
            pltpu.VMEM((2, 2 * head, rows), bf16),
            pltpu.VMEM((heads * rows, 2 * head), jnp.float32),
            pltpu.VMEM((slots, width + SKEW), bf16),
            pltpu.VMEM((slots, ff + SKEW), bf16),
            pltpu.VMEM((n_tp * heads * head, width - narrow + SKEW), bf16),
            pltpu.VMEM((n_tp, piece, heads * head), bf16),
            pltpu.VMEM((n_tp, piece, heads * head), bf16),
            pltpu.VMEM((piece, width - narrow), jnp.float32),
            pltpu.VMEM((ny, piece, narrow), bf16),
            pltpu.VMEM((ny, piece, narrow), bf16),
            pltpu.VMEM((ny, piece, narrow), bf16),
            pltpu.VMEM((ny, piece, narrow), bf16),
            pltpu.VMEM((2, 2, ny, slots // 2, dq), bf16),
            pltpu.VMEM((2, ny, slots // 2, dq), bf16),
            pltpu.VMEM((2, ny, slots // 2, dq), bf16),
            pltpu.VMEM((2, ny, slots // 2, dq), bf16),
            pltpu.VMEM((slots, dq), bf16),
            pltpu.VMEM((slots, dq), bf16),
            dma((13,)), dma((3,)),
            dma((nz + 1,)), dma((nz,)), dma((nz,)), dma((nz,)),
            dma((n_ep,)), dma((n_ep,)), dma((n_ep, ny)), dma((n_ep, ny)),
            dma((2,)), dma((2,)), dma((2, ny)), dma((2, ny)),
            dma((1,)), dma((1,)), dma((ny, strips)), dma((ny, strips)), dma((ny,)), dma((ny,)), dma((n_tp,)), dma((n_tp,)),
            dma((ny,)), dma((ny,)), dma((ny, 2)), dma((ny, 2)),
            dma((2,)), dma((2,)), dma((2, 2, ny)), dma((2, 2, ny)),
            dma((n_ep,)), dma((n_ep,)),
        ],
        compiler_params=pltpu.CompilerParams(
            collective_id=0, has_side_effects=True, vmem_limit_bytes=VMEM_LIMIT
        ),
    )(
        routes.T, route_logits.T, pre_gain[None, :], post_gain[None, :], q_gain[None, :], k_gain[None, :], turns,
        q_in, k_in, v_in, moe_in, w_out, w_gate[0], w_up[0], w_down[0],
    )


def solution(mesh):
    return jax.shard_map(
        functools.partial(per_device, mesh.shape["ep"], mesh.shape["tp"]),
        mesh=mesh,
        in_specs=(
            P("ep", "tp"),
            P("ep", None),
            P("ep", None),
            P(),
            P(),
            P("tp", None),
            P(),
            P("ep", None),
            P("ep", None),
            P("ep", None),
            P(),
            P("ep", None, "tp"),
            P("ep", None, "tp"),
            P("ep", "tp", None),
        ),
        out_specs=(P(("ep", "tp"), None), P("ep", "tp")),
        check_vma=False,
    )
```

```python
import functools

import jax
import jax.numpy as jnp
import numpy as np
from jax import lax
from jax.experimental import pallas as pl
from jax.experimental.pallas import tpu as pltpu
from jax.sharding import PartitionSpec as P

GRID_W = 128
EPSILON = 1e-06
ROPE_BASE = 10000.0
MESH = pl.DeviceIdType.MESH
SKEW = 128
VMEM_LIMIT = 60 * 1024 * 1024


def turn_tables(positions, rows_of_grid, quarter):
    inverse = ROPE_BASE ** (-np.arange(quarter, dtype=np.float32) / np.float32(quarter))
    inverse = inverse.astype(np.float32)

    def table(count, first_half):
        angles = (np.arange(count, dtype=np.float32)[:, None] * inverse[None, :]).astype(np.float64)
        cos, sin = np.cos(angles), np.sin(angles)
        none = np.zeros_like(cos)
        cos = np.concatenate([cos, cos, none, none] if first_half else [none, none, cos, cos], axis=1)
        sin = np.concatenate([-sin, sin, none, none] if first_half else [none, none, -sin, sin], axis=1)
        return np.concatenate([cos, cos], axis=1), np.concatenate([sin, sin], axis=1)

    grid_rows = positions // rows_of_grid
    by_row = table(grid_rows, True)
    by_col = table(rows_of_grid, False)
    return jnp.asarray(np.concatenate(by_row + by_col), jnp.float32)


def kernel(
    dims,
    route_hbm, logit_hbm, pre_hbm, gain_hbm, qg_hbm, kg_hbm, turn_hbm,
    q_hbm, k_hbm, v_hbm, x_hbm, wout_hbm, wg_hbm, wu_hbm, wd_hbm,
    attn_ref, moe_ref,
    route_ref, logit_ref, pre_ref, gain_ref, qg_ref, kg_ref, turn_ref,
    q_in, k_in, v_in, x_ref, wout_ref, q_ref, placed_ref,
    outgo_ref, mixw_ref, wg, wu, wd, kvbuf, vx, kt, acc, arrived, hidden,
    mix_high, mix_low, wall, ho_out, ho_in, whole, pa, pa_in, pa_red, pa_in2, pm, pm_in, pm_red, pm_in2, summed, ret,
    in_sem, w_sem, kz_s, kz_r, kx_s, kx_r, disp_s, disp_r, rel_s, rel_r, c0_s, c0_r, cy_s, cy_r,
    w0_s, w0_r, wy_s, wy_r, wc_s, wc_r, ho_s, ho_r, a1_s, a1_r, a2_s, a2_r, m1_s, m1_r, m2_s, m2_r, ret_s, ret_r,
):
    n_ep, n_tp, heads, cap, repeat = dims
    ny = n_tp // 2
    nz = n_ep // 2
    ep = lax.axis_index("ep")
    tp = lax.axis_index("tp")
    core = lax.rem(tp, 2)
    row = lax.div(tp, 2)
    partner = row * 2 + 1 - core
    side = lax.rem(ep, 2)
    col = lax.div(ep, 2)
    mate = col * 2 + 1 - side
    rows_kv = k_in.shape[0]
    dq = outgo_ref.shape[1]
    slots = outgo_ref.shape[0]
    piece = attn_ref.shape[0]
    bf16, f32 = jnp.bfloat16, jnp.float32

    def remote(src, dst, ss, rs, e, t):
        return pltpu.make_async_remote_copy(
            src_ref=src, dst_ref=dst, send_sem=ss, recv_sem=rs,
            device_id=(e, t), device_id_type=MESH,
        )

    def wait(name, copy):
        with jax.named_scope(name):
            copy.wait_recv()

    def ep_at(d):
        return lax.rem(ep + d, n_ep)

    def flip(d):
        other = ep
        for bit in range(n_ep.bit_length() - 1):
            if (d >> bit) % 2:
                other = other + (1 << bit) * (1 - 2 * lax.rem(lax.div(ep, 1 << bit), 2))
        return other

    def same_core(d):
        return lax.rem(row + d, ny) * 2 + core

    def row_from(d):
        return lax.rem(row - d + ny, ny)

    def slot_rows(e):
        return pl.ds(pl.multiple_of(e * cap, cap), cap)

    def cols_of(ref):
        return pl.ds(0, ref.shape[1])

    narrow = pa.shape[2]
    wide = wout_hbm.shape[1] - narrow
    dims_here = wout_hbm.shape[0]
    parts = min(8, dims_here // 16)
    strip = dims_here // parts
    starts = (parts * 5 // 8, parts * 7 // 8)

    def wall_rows(t, i, count):
        first_row = pl.multiple_of(t * dims_here + i * strip, strip)
        return wall.at[pl.ds(first_row, count * strip), pl.ds(0, wide)]

    def w_partner():
        block = wall_rows(tp, 0, parts)
        return remote(block, block, w0_s.at[0], w0_r.at[0], ep, partner)

    def w_row(dy, i):
        block = wall_rows(tp, i, 1)
        return remote(block, block, wy_s.at[dy - 1], wy_r.at[dy - 1], ep, same_core(dy))

    def w_row_all(dy):
        block = wall_rows(tp, 0, parts)
        return remote(block, block, wy_s.at[dy - 1], wy_r.at[dy - 1], ep, same_core(dy))

    def w_cross(dy):
        block = wall_rows(row_from(dy) * 2 + core, 0, parts)
        return remote(block, block, wc_s.at[dy - 1], wc_r.at[dy - 1], ep, partner)

    def w_send(i):
        for dy in range(1, ny):
            w_row(dy, i).start()

    def lanes_of(t):
        return pl.ds(pl.multiple_of(t * dq, dq), dq)

    quarter = n_ep // 4
    near = list(range(quarter - 1, -1, -1))
    groups = [
        list(range(2 * quarter, 3 * quarter)) + near,
        list(range(3 * quarter, 4 * quarter)) + list(range(quarter, 2 * quarter)),
    ]
    order = groups[0] + groups[1]
    chunk = slots // 2
    part = chunk // 2

    def held(d):
        return pl.ds(order.index(d) * cap, cap)

    head = qg_hbm.shape[1]
    lane_count = 2 * head
    kv_index = lax.div(tp * heads, repeat)
    kv_lanes = pl.ds(pl.multiple_of(lax.div(kv_index, 2) * lane_count, lane_count), lane_count)
    ins = [
        pltpu.make_async_copy(src, dst, in_sem.at[i])
        for i, (src, dst) in enumerate((
            (route_hbm, route_ref), (logit_hbm, logit_ref), (x_hbm, x_ref), (pre_hbm, pre_ref),
            (k_hbm.at[:, kv_lanes], k_in), (v_hbm.at[:, kv_lanes], v_in), (turn_hbm, turn_ref), (kg_hbm, kg_ref),
            (q_hbm, q_in), (qg_hbm, qg_ref), (gain_hbm, gain_ref), (wout_hbm.at[:, pl.ds(0, narrow)], wout_ref.at[:, pl.ds(0, narrow)]),
            (wout_hbm.at[:, pl.ds(narrow, wide)], wall_rows(tp, 0, parts)),
        ))
    ]
    for copy in ins:
        copy.start()
    loads = [
        pltpu.make_async_copy(src, dst, w_sem.at[i])
        for i, (src, dst) in enumerate(((wg_hbm, wg.at[:, cols_of(wg_hbm)]), (wu_hbm, wu.at[:, cols_of(wu_hbm)]), (wd_hbm, wd.at[:, cols_of(wd_hbm)])))
    ]
    for copy in loads:
        copy.start()
    barrier = pltpu.get_barrier_semaphore()
    for d in range(1, n_ep):
        pl.semaphore_signal(barrier, inc=1, device_id=(ep_at(d), tp), device_id_type=MESH)
    for d in range(1, ny):
        pl.semaphore_signal(barrier, inc=1, device_id=(ep, same_core(d)), device_id_type=MESH)
    pl.semaphore_signal(barrier, inc=1, device_id=(ep, partner), device_id_type=MESH)

    top, tokens = logit_ref.shape
    ins[0].wait()
    ins[1].wait()
    logits = logit_ref[...]
    power = jnp.exp(logits - jnp.max(logits, axis=0, keepdims=True))
    chance = power / jnp.sum(power, axis=0, keepdims=True)
    expert = lax.broadcasted_iota(jnp.int32, (n_ep, tokens), 0)
    named = jnp.zeros((n_ep, tokens), f32)
    share = jnp.zeros((n_ep, tokens), f32)
    for j in range(top):
        hit = route_ref[j : j + 1, :] == expert
        named = jnp.where(hit, 1.0, named)
        share = jnp.where(hit, chance[j : j + 1, :], share)
    above = lax.broadcasted_iota(jnp.int32, (tokens, tokens), 0) < lax.broadcasted_iota(
        jnp.int32, (tokens, tokens), 1
    )
    rank = jnp.dot(named, jnp.where(above, 1.0, 0.0), preferred_element_type=f32)
    rank = jnp.where(named > 0.0, rank, -1.0)
    place = lax.broadcasted_iota(jnp.int32, (cap, tokens), 0).astype(f32)
    for e in range(n_ep):
        there = rank[e : e + 1, :] == place
        placed_ref[e * cap : (e + 1) * cap, :] = jnp.where(there, 1.0, 0.0).astype(bf16)
        mixw_ref[e * cap : (e + 1) * cap, :] = jnp.where(there, share[e : e + 1, :], 0.0)

    ins[2].wait()
    ins[3].wait()
    x = x_ref[...].astype(f32)
    scale = lax.rsqrt(jnp.mean(x * x, axis=-1, keepdims=True) + EPSILON)
    mine = pl.ds(pl.multiple_of(tp * dq, dq), dq)
    normed = (x_ref[:, mine].astype(f32) * scale * pre_ref[:, mine]).astype(bf16)
    outgo_ref[...] = jnp.dot(placed_ref[...], normed, preferred_element_type=f32).astype(bf16)

    lane = lax.broadcasted_iota(jnp.int32, (GRID_W, lane_count), 1)
    first = lane < head
    ahead = lax.rem(lane, head // 2) < head // 4
    joined = lax.broadcasted_iota(jnp.int32, (lane_count, lane_count), 0) // head == (
        lax.broadcasted_iota(jnp.int32, (lane_count, lane_count), 1) // head
    )
    joined = jnp.where(joined, 1.0, 0.0).astype(bf16)
    blocks = rows_kv // GRID_W

    def turned(values, gain, b):
        square = values * values
        high = square.astype(bf16)
        low = (square - high.astype(f32)).astype(bf16)
        total = jnp.dot(high, joined, preferred_element_type=f32) + jnp.dot(
            low, joined, preferred_element_type=f32
        )
        values = values * lax.rsqrt(total * (1.0 / head) + EPSILON) * gain
        other = jnp.where(
            ahead,
            pltpu.roll(values, lane_count - head // 4, 1),
            pltpu.roll(values, head // 4, 1),
        )
        lines = turn_ref.shape[0] // 2 - GRID_W
        cos = turn_ref[pl.ds(ep * blocks + b, 1), :] + turn_ref[2 * lines : 2 * lines + GRID_W, :]
        sin = turn_ref[pl.ds(lines + ep * blocks + b, 1), :] + turn_ref[2 * lines + GRID_W :, :]
        return values * cos + other * sin

    odd = lax.rem(kv_index, 2)
    for copy in ins[4:8]:
        copy.wait()
    k_gain = jnp.concatenate([kg_ref[...], kg_ref[...]], axis=1)
    for b in range(blocks):
        at = slice(b * GRID_W, (b + 1) * GRID_W)
        keys = turned(k_in[at, :].astype(f32), k_gain, b)
        keys = jnp.where(odd == 1, pltpu.roll(keys, head, 1), keys)
        values = v_in[at, :].astype(f32)
        values = jnp.where(odd == 1, values, pltpu.roll(values, head, 1))
        kvbuf[ep, at, :] = jnp.where(first, keys, values).astype(bf16)
    with jax.named_scope("barrier"):
        pl.semaphore_wait(barrier, n_ep - 1 + ny - 1 + 1)

    disp = {
        d: remote(outgo_ref.at[slot_rows(flip(d))], arrived.at[held(d), lanes_of(tp)],
                  disp_s.at[0], disp_r.at[d - 1], flip(d), tp)
        for d in range(1, n_ep)
    }

    def kv_line(b, target, sem):
        block = kvbuf.at[b * 2 + side]
        return remote(block, block, kz_s.at[sem], kz_r.at[b], target * 2 + side, tp)

    def kv_pass(b):
        block = kvbuf.at[b * 2 + side]
        return remote(block, block, kx_s.at[b], kx_r.at[b], mate, tp)

    has_next = col < nz - 1
    has_prev = col > 0

    for d in groups[0]:
        if d:
            disp[d].start()
    kv_pass(col).start()

    @pl.when(has_next)
    def _():
        kv_line(col, col + 1, col).start()

    @pl.when(has_prev)
    def _():
        kv_line(col, col - 1, nz).start()

    for d in groups[1]:
        disp[d].start()
    ins[12].wait()
    for i in range(starts[0]):
        w_send(i)
    w_partner().start()
    ins[8].wait()
    ins[9].wait()
    q_gain = jnp.concatenate([qg_ref[...], qg_ref[...]], axis=1)
    for g in range(max(1, heads // 2)):
        for b in range(blocks):
            at = slice(b * GRID_W, (b + 1) * GRID_W)
            if heads == 1:
                values = q_in[at, :].astype(f32)
                values = jnp.concatenate([values, jnp.zeros_like(values)], axis=1)
            else:
                values = q_in[at, g * lane_count : (g + 1) * lane_count].astype(f32)
            values = turned(values, q_gain, b) * (head ** (-0.5))
            for h in range(min(2, heads)):
                one = values if h == 0 else pltpu.roll(values, head, 1)
                one = jnp.where(first, one, 0.0).astype(bf16)
                for i in range(max(1, GRID_W // piece)):
                    size = min(piece, GRID_W)
                    token = b * GRID_W + i * size
                    row_at = (token // piece * heads + 2 * g + h) * piece + token % piece
                    q_ref[row_at : row_at + size, :] = one[i * size : (i + 1) * size, :]

    mine_rows = placed_ref[slot_rows(ep), :]
    for q in range(n_tp):
        at = slice(q * dq, (q + 1) * dq)
        full = (x_ref[:, at].astype(f32) * scale * pre_ref[:, at]).astype(bf16)
        arrived[held(0), at] = jnp.dot(mine_rows, full, preferred_element_type=f32).astype(bf16)

    q_rows = q_ref.shape[0]
    tile = min(512, heads * piece)

    def prepare(e, slot):
        keys = kvbuf[e]
        lanes = lax.broadcasted_iota(jnp.int32, keys.shape, 1)
        kt[slot] = keys.T
        vx[slot] = jnp.where(lanes < keys.shape[1] // 2, jnp.ones_like(keys), keys)

    def attend_rows(i, slot, fresh):
        for sub in range(2):
            at = pl.ds(pl.multiple_of(i * 2 * tile + sub * tile, tile), tile)
            scores = jnp.dot(q_ref[at, :], kt[slot], preferred_element_type=f32)
            weights = jnp.exp(scores).astype(bf16)
            term = jnp.dot(weights, vx[slot], preferred_element_type=f32)
            if fresh:
                acc[at, :] = term
            else:
                acc[at, :] += term

    def attend(e, fresh):
        prepare(e, 0)

        for i in range(q_rows // (2 * tile)):
            attend_rows(i, 0, fresh)

    shorter = jnp.minimum(col, nz - 1 - col)
    longer = jnp.where(col <= nz - 1 - col, 1, -1)

    def line_step(k):
        both = k < 2 * shorter
        way = jnp.where(both, 2 * lax.rem(k, 2) - 1, longer)
        far = jnp.where(both, lax.div(k, 2) + 1, k - shorter + 1)
        return col + way * far, col - way

    def line_one(k):
        b, target = line_step(k)
        wait("kv_line", kv_line(b, target, b))

        @pl.when(jnp.logical_and(target >= 0, target <= nz - 1))
        def _():
            kv_line(b, target, b).start()

        kv_pass(b).start()

    def line_take(k):
        both = k < 2 * shorter
        opening = jnp.logical_or(lax.rem(k, 2) == 0, jnp.logical_not(both))

        @pl.when(opening)
        def _():
            line_one(k)

        @pl.when(jnp.logical_and(opening, both))
        def _():
            line_one(k + 1)

    def line_end(early):
        middle = shorter > 0

        @pl.when(middle if early else jnp.logical_not(middle))
        def _():
            line_one(nz - 1 - 1)

    def line_block(k):
        return line_step(k)[0] * 2 + side

    def pass_block(k):
        b, _ = line_step(k)
        wait("kv_pass", kv_pass(b))
        return b * 2 + 1 - side

    def take(k, carry):
        line_take(k)
        attend(line_block(k), False)
        attend(pass_block(k), False)
        return carry

    def relay(d, dy):
        block = arrived.at[held(d), lanes_of(tp)]
        c = 0 if d in groups[0] else 1
        return remote(block, block, rel_s.at[c, dy - 1], rel_r.at[c, dy - 1], ep, same_core(dy))

    def relay_all(c, dy):
        block = arrived.at[foreign(c), lanes_of(row_from(dy) * 2 + core)]
        return remote(block, block, rel_s.at[c, dy - 1], rel_r.at[c, dy - 1], ep, same_core(dy))

    def foreign(c):
        count = len(groups[c]) - (1 if 0 in groups[c] else 0)
        return pl.ds(c * chunk, count * cap)

    def cross(c, dy):
        block = arrived.at[foreign(c), lanes_of(row_from(dy) * 2 + core)]
        if dy == 0:
            return remote(block, block, c0_s.at[c], c0_r.at[c], ep, partner)
        return remote(block, block, cy_s.at[c, dy - 1], cy_r.at[c, dy - 1], ep, partner)

    def relay_chunk(c):
        for d in groups[c]:
            if d:
                wait("disp", disp[d])
                for dy in range(1, ny):
                    relay(d, dy).start()
        cross(c, 0).start()

    def cross_chunk(c):
        for dy in range(1, ny):
            wait("relay", relay_all(c, dy))
            cross(c, dy).start()

    ff = wg_hbm.shape[1]
    step = min(512, ff)

    def m1(c):
        return remote(pm.at[c, 1 - core], pm_in.at[c], m1_s.at[c], m1_r.at[c], ep, partner)

    def m2(c, s, dy):
        at = pl.ds(s * part, part)
        return remote(pm_red.at[c, lax.rem(row + dy, ny), at], pm_in2.at[c, row, at],
                      m2_s.at[c, dy - 1], m2_r.at[c, s, dy - 1], ep, same_core(dy))

    def chunk_rows(c):
        return slice(c * chunk, (c + 1) * chunk)

    def m2_all(c, dy):
        return remote(pm_red.at[c, row], pm_in2.at[c, row], m2_s.at[c, dy - 1], m2_r.at[c, 0, dy - 1], ep, partner)

    def experts_up(c):
        for dy in range(ny):
            wait("cross", cross(c, dy))
        if c == 0:
            loads[0].wait()
            loads[1].wait()
        rows = chunk_rows(c)

        def gated(i, carry):
            at = pl.ds(pl.multiple_of(i * step, step), step)
            x = arrived[rows, : wg_hbm.shape[0]]
            gate = jnp.dot(x, wg[:, at], preferred_element_type=f32)
            up = jnp.dot(x, wu[:, at], preferred_element_type=f32)
            hidden[rows, at] = (gate / (1.0 + jnp.exp(-gate)) * up).astype(bf16)
            return carry

        lax.fori_loop(0, ff // step, gated, 0)

    def experts_down(c):
        rows = chunk_rows(c)
        if c == 0:
            loads[2].wait()

        def down_for(which):
            for y in range(ny):
                cols = pl.ds(pl.multiple_of((y * 2 + which) * dq, dq), dq)
                pm[c, which, y] = jnp.dot(
                    hidden[rows, :ff], wd[:, cols], preferred_element_type=f32
                ).astype(bf16)

        down_for(1 - core)
        m1(c).start()
        down_for(core)

    def reduce_cores(c):
        wait("m1", m1(c))
        for y in range(ny):
            pm_red[c, y] = (pm[c, core, y].astype(f32) + pm_in[c, y].astype(f32)).astype(bf16)
        for s in range(2):
            for dy in range(1, ny):
                m2(c, s, dy).start()

    def back(d):
        return remote(summed.at[held(d)], ret.at[slot_rows(ep)], ret_s.at[0], ret_r.at[0], flip(d), tp)

    def back_all():
        at = pl.ds(0, (n_ep - 1) * cap)
        return remote(summed.at[at], ret.at[at], ret_s.at[0], ret_r.at[0], mate, tp)

    def disp_all():
        at = pl.ds(0, (n_ep - 1) * cap)
        return remote(outgo_ref.at[at], summed.at[at], disp_s.at[0], disp_r.at[0], mate, tp)

    def send_back(c):
        for s in range(2):
            for dy in range(1, ny):
                wait("m2", m2(c, s, dy))
            at = slice(s * part, (s + 1) * part)
            total = pm_red[c, row, at].astype(f32)
            for dy in range(1, ny):
                total = total + pm_in2[c, row_from(dy), at].astype(f32)
            total = total.astype(bf16)
            rows_at = c * chunk + s * part
            summed[rows_at : rows_at + part, :] = total
            for d in order[rows_at // cap : (rows_at + part) // cap]:
                if d:
                    back(d).start()
                else:
                    low = order.index(0) * cap - rows_at
                    ret[slot_rows(ep), :] = total[low : low + cap, :]

    tall = heads * piece
    half = acc.shape[1] // 2

    def finish(target):
        for slot in range(2):
            for i in range(2 * tall // (2 * tile)):
                attend_rows(target * (tall // tile) + i, slot, False)
        sides = []
        for c in range(2):
            which = core if c else 1 - core
            pieces = []
            for h in range(heads):
                at = pl.ds(pl.multiple_of((target * 2 + which) * tall + h * piece, piece), piece)
                sums = acc[at, :]
                pieces.append((sums[:, half:] / sums[:, :half]).astype(bf16))
            sides.append(pieces[0] if heads == 1 else jnp.concatenate(pieces, axis=1))
        return sides

    def a1(d):
        return remote(pa.at[d], pa_in.at[d], a1_s.at[d], a1_r.at[d], ep, partner)

    def a2(d, s):
        at = pl.ds(s * (piece // 2), piece // 2)
        return remote(pa_red.at[d, at], pa_in2.at[d, at], a2_s.at[d - 1], a2_r.at[d - 1, s], ep, same_core(d))

    def a2_all(d):
        return remote(pa_red.at[d], pa_in2.at[d], a2_s.at[d - 1], a2_r.at[d - 1, 0], ep, same_core(d))

    def ho(d, c):
        target = lax.rem(row + d, ny) * 2 + (core if c else 1 - core)
        return remote(ho_out.at[2 * d + c], ho_in.at[tp], ho_s.at[0], ho_r.at[0], ep, target)

    def ho_all():
        block = ho_out.at[pl.ds(0, n_tp - 1)]
        return remote(block, ho_in.at[pl.ds(0, n_tp - 1)], ho_s.at[0], ho_r.at[0], ep, partner)

    def finish_start(d):
        sides = finish(lax.rem(row + d, ny))
        for c in range(2):
            if d == 0 and c == 1:
                ho_in[tp] = sides[1]
            else:
                ho_out[2 * d + c] = sides[c]
                ho(d, c).start()
        both = jnp.concatenate(sides, axis=0)
        total = jnp.dot(both, wout_ref[:, :narrow], preferred_element_type=f32).astype(bf16)
        pa[d] = total[:piece]
        a1(d).start()
        pa_red[d] = total[piece:]

    def finish_end(d):
        wait("a1", a1(d))
        return pa_red[d].astype(f32) + pa_in[d].astype(f32)

    attend(ep, True)
    mixw = mixw_ref[...].T
    high = mixw.astype(bf16)
    mix_high[...] = high
    mix_low[...] = (mixw - high.astype(f32)).astype(bf16)
    relay_chunk(0)
    wait("kv_mate", kv_pass(col))
    attend(mate, False)
    split = max(1, (nz - 1) // 2)
    brief = nz - 2 == split + 1
    line_take(0)
    attend(line_block(0), False)
    relay_chunk(1)
    for i in range(*starts):
        w_send(i)
    cross_chunk(0)
    attend(pass_block(0), False)
    lax.fori_loop(1, split, take, 0)
    if brief:
        line_end(True)
    with jax.named_scope("up0"):
        experts_up(0)
    line_take(split)
    with jax.named_scope("down0"):
        experts_down(0)
    cross_chunk(1)
    attend(line_block(split), False)
    reduce_cores(0)
    for i in range(starts[1], parts):
        w_send(i)
    with jax.named_scope("up1"):
        experts_up(1)
    if brief:
        line_end(False)
    with jax.named_scope("down1"):
        experts_down(1)
    attend(pass_block(split), False)
    lax.fori_loop(split + 1, nz - 2, take, 0)
    if not brief:
        line_take(nz - 2)
    reduce_cores(1)
    prepare(line_block(nz - 2), 0)
    prepare(pass_block(nz - 2), 1)
    ins[10].wait()
    ins[11].wait()
    for d in range(1, ny):
        with jax.named_scope("finish"):
            finish_start(d)
    send_back(0)
    for dy in range(1, ny):
        wait("w_row", w_row_all(dy))
        w_cross(dy).start()
    for d in range(1, ny):
        pa_red[d] = finish_end(d).astype(bf16)
        for s in range(2):
            a2(d, s).start()
    with jax.named_scope("finish"):
        finish_start(0)
    send_back(1)
    pa_red[0] = finish_end(0).astype(bf16)
    wait("w_partner", w_partner())
    for dy in range(1, ny):
        wait("w_cross", w_cross(dy))
    wait("ho", ho_all())
    gathered = jnp.concatenate([ho_in[t] for t in range(n_tp)], axis=1)
    whole[...] = jnp.dot(gathered, wall[:, :wide], preferred_element_type=f32)
    for s in range(2):
        at = slice(s * (piece // 2), (s + 1) * (piece // 2))
        mixed = pa_red[0, at].astype(f32)
        for d in range(1, ny):
            wait("a2", a2(d, s))
            mixed = mixed + pa_in2[d, at].astype(f32)
        rest = whole[at, :]
        square = jnp.sum(mixed * mixed, axis=-1, keepdims=True) + jnp.sum(rest * rest, axis=-1, keepdims=True)
        scale = lax.rsqrt(square * (1.0 / (narrow + wide)) + EPSILON)
        attn_ref[at, :narrow] = (mixed * scale * gain_ref[:, :narrow]).astype(bf16)
        attn_ref[at, narrow:] = (rest * scale * gain_ref[:, narrow:]).astype(bf16)

    wait("back", back_all())
    moe_ref[...] = (
        jnp.dot(mix_high[...], ret[...], preferred_element_type=f32)
        + jnp.dot(mix_low[...], ret[...], preferred_element_type=f32)
    ).astype(bf16)

    sent = [kv_pass(col), disp_all(), back_all(), ho_all(), w_partner()]
    sent += [relay_all(c, dy) for c in range(2) for dy in range(1, ny)]
    sent += [cross(c, dy) for c in range(2) for dy in range(ny)]
    sent += [m1(c) for c in range(2)]
    sent += [m2_all(c, dy) for c in range(2) for dy in range(1, ny)]
    sent += [w_row_all(dy) for dy in range(1, ny)]
    sent += [w_cross(dy) for dy in range(1, ny)]
    sent += [a1(d) for d in range(ny)] + [a2_all(d) for d in range(1, ny)]
    for copy in sent:
        copy.wait_send()

    @pl.when(has_next)
    def _():
        kv_line(col, col + 1, col).wait_send()

    @pl.when(has_prev)
    def _():
        kv_line(col, col - 1, nz).wait_send()

    def kv_done(k, carry):
        b, target = line_step(k)

        @pl.when(jnp.logical_and(target >= 0, target <= nz - 1))
        def _():
            kv_line(b, target, b).wait_send()

        kv_pass(b).wait_send()
        return carry

    lax.fori_loop(0, nz - 1, kv_done, 0)


def hand_over(attn_ref, moe_ref, attn_hbm, moe_hbm, sem):
    copies = [
        pltpu.make_async_copy(attn_ref, attn_hbm, sem.at[0]),
        pltpu.make_async_copy(moe_ref, moe_hbm, sem.at[1]),
    ]
    for copy in copies:
        copy.start()
    for copy in copies:
        copy.wait()


def per_device(
    n_ep, n_tp,
    q_in, k_in, v_in, q_gain, k_gain, w_out, post_gain,
    moe_in, routes, route_logits, pre_gain, w_gate, w_up, w_down,
):
    bf16 = jnp.bfloat16
    head = q_gain.shape[0]
    rows = q_in.shape[0]
    heads = q_in.shape[1] // head
    kv_count = k_in.shape[1] // head
    repeat = heads * n_tp // kv_count
    ny = n_tp // 2
    nz = n_ep // 2
    turns = turn_tables(n_ep * rows, GRID_W, head // 4)

    tokens, top = routes.shape
    width = moe_in.shape[1]
    dq = width // n_tp
    need = max(2, 3 * top * tokens // (2 * n_ep))
    cap = -(-need // 16) * 16
    slots = n_ep * cap

    piece = rows // n_tp
    ff = w_gate.shape[2]
    narrow = width * 4 // 8
    dma = pltpu.SemaphoreType.DMA
    vmem = pl.BlockSpec(memory_space=pltpu.VMEM)
    hbm = pl.BlockSpec(memory_space=pl.ANY)
    outs = pl.pallas_call(
        functools.partial(kernel, (n_ep, n_tp, heads, cap, repeat)),
        out_shape=(
            pltpu.VMEM((piece, width), bf16),
            pltpu.VMEM((tokens, dq), bf16),
        ),
        in_specs=[hbm] * 15,
        out_specs=(vmem, vmem),
        scratch_shapes=[
            pltpu.VMEM((top, tokens), jnp.int32),
            pltpu.VMEM((top, tokens), jnp.float32),
            pltpu.VMEM((1, width), jnp.float32),
            pltpu.VMEM((1, width), jnp.float32),
            pltpu.VMEM((1, head), jnp.float32),
            pltpu.VMEM((1, head), jnp.float32),
            pltpu.VMEM(turns.shape, jnp.float32),
            pltpu.VMEM((rows, heads * head), bf16),
            pltpu.VMEM((rows, 2 * head), bf16),
            pltpu.VMEM((rows, 2 * head), bf16),
            pltpu.VMEM((tokens, width), bf16),
            pltpu.VMEM((heads * head, narrow + SKEW), bf16),
            pltpu.VMEM((heads * rows, 2 * head), bf16),
            pltpu.VMEM((slots, tokens), bf16),
            pltpu.VMEM((slots, dq), bf16),
            pltpu.VMEM((slots, tokens), jnp.float32),
            pltpu.VMEM((width, ff + SKEW), bf16),
            pltpu.VMEM((width, ff + SKEW), bf16),
            pltpu.VMEM((ff, width + SKEW), bf16),
            pltpu.VMEM((n_ep, rows, 2 * head), bf16),
            pltpu.VMEM((2, rows, 2 * head), bf16),
            pltpu.VMEM((2, 2 * head, rows), bf16),
            pltpu.VMEM((heads * rows, 2 * head), jnp.float32),
            pltpu.VMEM((slots, width + SKEW), bf16),
            pltpu.VMEM((slots, ff + SKEW), bf16),
            pltpu.VMEM((tokens, slots), bf16),
            pltpu.VMEM((tokens, slots), bf16),
            pltpu.VMEM((n_tp * heads * head, width - narrow + SKEW), bf16),
            pltpu.VMEM((n_tp, piece, heads * head), bf16),
            pltpu.VMEM((n_tp, piece, heads * head), bf16),
            pltpu.VMEM((piece, width - narrow), jnp.float32),
            pltpu.VMEM((ny, piece, narrow), bf16),
            pltpu.VMEM((ny, piece, narrow), bf16),
            pltpu.VMEM((ny, piece, narrow), bf16),
            pltpu.VMEM((ny, piece, narrow), bf16),
            pltpu.VMEM((2, 2, ny, slots // 2, dq), bf16),
            pltpu.VMEM((2, ny, slots // 2, dq), bf16),
            pltpu.VMEM((2, ny, slots // 2, dq), bf16),
            pltpu.VMEM((2, ny, slots // 2, dq), bf16),
            pltpu.VMEM((slots, dq), bf16),
            pltpu.VMEM((slots, dq), bf16),
            dma((13,)), dma((3,)),
            dma((nz + 1,)), dma((nz,)), dma((nz,)), dma((nz,)),
            dma((1,)), dma((n_ep - 1,)), dma((2, ny - 1)), dma((2, ny - 1)),
            dma((2,)), dma((2,)), dma((2, ny - 1)), dma((2, ny - 1)),
            dma((1,)), dma((1,)), dma((ny - 1,)), dma((ny - 1,)), dma((ny - 1,)), dma((ny - 1,)), dma((1,)), dma((1,)),
            dma((ny,)), dma((ny,)), dma((ny - 1,)), dma((ny - 1, 2)),
            dma((2,)), dma((2,)), dma((2, ny - 1)), dma((2, 2, ny - 1)),
            dma((1,)), dma((1,)),
        ],
        compiler_params=pltpu.CompilerParams(
            collective_id=0, has_side_effects=True, vmem_limit_bytes=VMEM_LIMIT
        ),
    )(
        routes.T, route_logits.T, pre_gain[None, :], post_gain[None, :], q_gain[None, :], k_gain[None, :], turns,
        q_in, k_in, v_in, moe_in, w_out, w_gate[0], w_up[0], w_down[0],
    )
    return pl.pallas_call(
        hand_over,
        out_shape=(
            jax.ShapeDtypeStruct((piece, width), bf16),
            jax.ShapeDtypeStruct((tokens, dq), bf16),
        ),
        in_specs=[vmem, vmem],
        out_specs=(hbm, hbm),
        scratch_shapes=[dma((2,))],
        compiler_params=pltpu.CompilerParams(vmem_limit_bytes=2 * 1024 * 1024),
    )(*outs)


def solution(mesh):
    return jax.shard_map(
        functools.partial(per_device, mesh.shape["ep"], mesh.shape["tp"]),
        mesh=mesh,
        in_specs=(
            P("ep", "tp"),
            P("ep", None),
            P("ep", None),
            P(),
            P(),
            P("tp", None),
            P(),
            P("ep", None),
            P("ep", None),
            P("ep", None),
            P(),
            P("ep", None, "tp"),
            P("ep", None, "tp"),
            P("ep", "tp", None),
        ),
        out_specs=(P(("ep", "tp"), None), P("ep", "tp")),
        check_vma=False,
    )
```

```python
import functools

import jax
import jax.numpy as jnp
import numpy as np
from jax import lax
from jax.experimental import pallas as pl
from jax.experimental.pallas import tpu as pltpu
from jax.sharding import PartitionSpec as P

GRID_W = 128
EPSILON = 1e-06
ROPE_BASE = 10000.0
MESH = pl.DeviceIdType.MESH
SKEW = 128
VMEM_LIMIT = 60 * 1024 * 1024


def turn_tables(positions, rows_of_grid, quarter):
    inverse = ROPE_BASE ** (-np.arange(quarter, dtype=np.float32) / np.float32(quarter))
    inverse = inverse.astype(np.float32)

    def table(count, first_half):
        angles = (np.arange(count, dtype=np.float32)[:, None] * inverse[None, :]).astype(np.float64)
        cos, sin = np.cos(angles), np.sin(angles)
        none = np.zeros_like(cos)
        cos = np.concatenate([cos, cos, none, none] if first_half else [none, none, cos, cos], axis=1)
        sin = np.concatenate([-sin, sin, none, none] if first_half else [none, none, -sin, sin], axis=1)
        return np.concatenate([cos, cos], axis=1), np.concatenate([sin, sin], axis=1)

    grid_rows = positions // rows_of_grid
    by_row = table(grid_rows, True)
    by_col = table(rows_of_grid, False)
    return jnp.asarray(np.concatenate(by_row + by_col), jnp.float32)


def kernel(
    dims,
    route_hbm, logit_hbm, pre_hbm, gain_hbm, qg_hbm, kg_hbm, turn_hbm,
    q_hbm, k_hbm, v_hbm, x_hbm, wout_hbm, wg_hbm, wu_hbm, wd_hbm,
    attn_ref, moe_ref,
    route_ref, logit_ref, pre_ref, gain_ref, qg_ref, kg_ref, turn_ref,
    q_in, k_in, v_in, x_ref, wout_ref, q_ref, placed_ref,
    outgo_ref, mixw_ref, wg, wu, wd, kvbuf, vx, kt, acc, arrived, hidden,
    mix_high, mix_low, wall, ho_out, ho_in, whole, pa, pa_in, pa_red, pa_in2, pm, pm_in, pm_red, pm_in2, summed, ret,
    in_sem, w_sem, kz_s, kz_r, kx_s, kx_r, disp_s, disp_r, rel_s, rel_r, c0_s, c0_r, cy_s, cy_r,
    w0_s, w0_r, wy_s, wy_r, wc_s, wc_r, ho_s, ho_r, a1_s, a1_r, a2_s, a2_r, m1_s, m1_r, m2_s, m2_r, ret_s, ret_r,
):
    n_ep, n_tp, heads, cap, repeat = dims
    ny = n_tp // 2
    nz = n_ep // 2
    ep = lax.axis_index("ep")
    tp = lax.axis_index("tp")
    core = lax.rem(tp, 2)
    row = lax.div(tp, 2)
    partner = row * 2 + 1 - core
    side = lax.rem(ep, 2)
    col = lax.div(ep, 2)
    mate = col * 2 + 1 - side
    rows_kv = k_in.shape[0]
    dq = outgo_ref.shape[1]
    slots = outgo_ref.shape[0]
    piece = attn_ref.shape[0]
    bf16, f32 = jnp.bfloat16, jnp.float32

    def remote(src, dst, ss, rs, e, t):
        return pltpu.make_async_remote_copy(
            src_ref=src, dst_ref=dst, send_sem=ss, recv_sem=rs,
            device_id=(e, t), device_id_type=MESH,
        )

    def wait(name, copy):
        with jax.named_scope(name):
            copy.wait_recv()

    def ep_at(d):
        return lax.rem(ep + d, n_ep)

    def flip(d):
        other = ep
        for bit in range(n_ep.bit_length() - 1):
            if (d >> bit) % 2:
                other = other + (1 << bit) * (1 - 2 * lax.rem(lax.div(ep, 1 << bit), 2))
        return other

    def same_core(d):
        return lax.rem(row + d, ny) * 2 + core

    def row_from(d):
        return lax.rem(row - d + ny, ny)

    def slot_rows(e):
        return pl.ds(pl.multiple_of(e * cap, cap), cap)

    def cols_of(ref):
        return pl.ds(0, ref.shape[1])

    narrow = pa.shape[2]
    wide = wout_hbm.shape[1] - narrow
    dims_here = wout_hbm.shape[0]
    parts = min(8, dims_here // 16)
    strip = dims_here // parts
    starts = (parts * 4 // 8, parts * 8 // 8)

    def wall_rows(t, i, count):
        first_row = pl.multiple_of(t * dims_here + i * strip, strip)
        return wall.at[pl.ds(first_row, count * strip), pl.ds(0, wide)]

    def w_partner():
        block = wall_rows(tp, 0, parts)
        return remote(block, block, w0_s.at[0], w0_r.at[0], ep, partner)

    def w_row(dy, i):
        block = wall_rows(tp, i, 1)
        return remote(block, block, wy_s.at[dy - 1], wy_r.at[dy - 1], ep, same_core(dy))

    def w_row_all(dy):
        block = wall_rows(tp, 0, parts)
        return remote(block, block, wy_s.at[dy - 1], wy_r.at[dy - 1], ep, same_core(dy))

    def w_cross(dy):
        block = wall_rows(row_from(dy) * 2 + core, 0, parts)
        return remote(block, block, wc_s.at[dy - 1], wc_r.at[dy - 1], ep, partner)

    def w_send(i):
        for dy in range(1, ny):
            w_row(dy, i).start()

    def lanes_of(t):
        return pl.ds(pl.multiple_of(t * dq, dq), dq)

    quarter = n_ep // 4
    near = list(range(quarter - 1, -1, -1))
    groups = [
        list(range(2 * quarter, 3 * quarter)) + near,
        list(range(3 * quarter, 4 * quarter)) + list(range(quarter, 2 * quarter)),
    ]
    order = groups[0] + groups[1]
    chunk = slots // 2
    part = chunk // 2

    def held(d):
        return pl.ds(order.index(d) * cap, cap)

    head = qg_hbm.shape[1]
    lane_count = 2 * head
    kv_index = lax.div(tp * heads, repeat)
    kv_lanes = pl.ds(pl.multiple_of(lax.div(kv_index, 2) * lane_count, lane_count), lane_count)
    ins = [
        pltpu.make_async_copy(src, dst, in_sem.at[i])
        for i, (src, dst) in enumerate((
            (route_hbm, route_ref), (logit_hbm, logit_ref), (x_hbm, x_ref), (pre_hbm, pre_ref),
            (k_hbm.at[:, kv_lanes], k_in), (v_hbm.at[:, kv_lanes], v_in), (turn_hbm, turn_ref), (kg_hbm, kg_ref),
            (q_hbm, q_in), (qg_hbm, qg_ref), (gain_hbm, gain_ref), (wout_hbm.at[:, pl.ds(0, narrow)], wout_ref.at[:, pl.ds(0, narrow)]),
            (wout_hbm.at[:, pl.ds(narrow, wide)], wall_rows(tp, 0, parts)),
        ))
    ]
    for copy in ins[:8] + ins[12:]:
        copy.start()
    loads = [
        pltpu.make_async_copy(src, dst, w_sem.at[i])
        for i, (src, dst) in enumerate(((wg_hbm, wg.at[:, cols_of(wg_hbm)]), (wu_hbm, wu.at[:, cols_of(wu_hbm)]), (wd_hbm, wd.at[:, cols_of(wd_hbm)])))
    ]
    barrier = pltpu.get_barrier_semaphore()
    for d in range(1, n_ep):
        pl.semaphore_signal(barrier, inc=1, device_id=(ep_at(d), tp), device_id_type=MESH)
    for d in range(1, ny):
        pl.semaphore_signal(barrier, inc=1, device_id=(ep, same_core(d)), device_id_type=MESH)
    pl.semaphore_signal(barrier, inc=1, device_id=(ep, partner), device_id_type=MESH)

    top, tokens = logit_ref.shape
    ins[0].wait()
    ins[1].wait()
    logits = logit_ref[...]
    power = jnp.exp(logits - jnp.max(logits, axis=0, keepdims=True))
    chance = power / jnp.sum(power, axis=0, keepdims=True)
    expert = lax.broadcasted_iota(jnp.int32, (n_ep, tokens), 0)
    named = jnp.zeros((n_ep, tokens), f32)
    share = jnp.zeros((n_ep, tokens), f32)
    for j in range(top):
        hit = route_ref[j : j + 1, :] == expert
        named = jnp.where(hit, 1.0, named)
        share = jnp.where(hit, chance[j : j + 1, :], share)
    above = lax.broadcasted_iota(jnp.int32, (tokens, tokens), 0) < lax.broadcasted_iota(
        jnp.int32, (tokens, tokens), 1
    )
    rank = jnp.dot(named, jnp.where(above, 1.0, 0.0), preferred_element_type=f32)
    rank = jnp.where(named > 0.0, rank, -1.0)
    place = lax.broadcasted_iota(jnp.int32, (cap, tokens), 0).astype(f32)
    for e in range(n_ep):
        there = rank[e : e + 1, :] == place
        placed_ref[e * cap : (e + 1) * cap, :] = jnp.where(there, 1.0, 0.0).astype(bf16)
        mixw_ref[e * cap : (e + 1) * cap, :] = jnp.where(there, share[e : e + 1, :], 0.0)

    ins[2].wait()
    ins[3].wait()
    x = x_ref[...].astype(f32)
    scale = lax.rsqrt(jnp.mean(x * x, axis=-1, keepdims=True) + EPSILON)
    mine = pl.ds(pl.multiple_of(tp * dq, dq), dq)
    normed = (x_ref[:, mine].astype(f32) * scale * pre_ref[:, mine]).astype(bf16)
    outgo_ref[...] = jnp.dot(placed_ref[...], normed, preferred_element_type=f32).astype(bf16)

    lane = lax.broadcasted_iota(jnp.int32, (GRID_W, lane_count), 1)
    first = lane < head
    ahead = lax.rem(lane, head // 2) < head // 4
    joined = lax.broadcasted_iota(jnp.int32, (lane_count, lane_count), 0) // head == (
        lax.broadcasted_iota(jnp.int32, (lane_count, lane_count), 1) // head
    )
    joined = jnp.where(joined, 1.0, 0.0).astype(bf16)
    blocks = rows_kv // GRID_W

    def turned(values, gain, b):
        square = values * values
        high = square.astype(bf16)
        low = (square - high.astype(f32)).astype(bf16)
        total = jnp.dot(high, joined, preferred_element_type=f32) + jnp.dot(
            low, joined, preferred_element_type=f32
        )
        values = values * lax.rsqrt(total * (1.0 / head) + EPSILON) * gain
        other = jnp.where(
            ahead,
            pltpu.roll(values, lane_count - head // 4, 1),
            pltpu.roll(values, head // 4, 1),
        )
        lines = turn_ref.shape[0] // 2 - GRID_W
        cos = turn_ref[pl.ds(ep * blocks + b, 1), :] + turn_ref[2 * lines : 2 * lines + GRID_W, :]
        sin = turn_ref[pl.ds(lines + ep * blocks + b, 1), :] + turn_ref[2 * lines + GRID_W :, :]
        return values * cos + other * sin

    odd = lax.rem(kv_index, 2)
    for copy in ins[4:8]:
        copy.wait()
    for copy in ins[8:12] + loads:
        copy.start()
    k_gain = jnp.concatenate([kg_ref[...], kg_ref[...]], axis=1)
    for b in range(blocks):
        at = slice(b * GRID_W, (b + 1) * GRID_W)
        keys = turned(k_in[at, :].astype(f32), k_gain, b)
        keys = jnp.where(odd == 1, pltpu.roll(keys, head, 1), keys)
        values = v_in[at, :].astype(f32)
        values = jnp.where(odd == 1, values, pltpu.roll(values, head, 1))
        kvbuf[ep, at, :] = jnp.where(first, keys, values).astype(bf16)
    with jax.named_scope("barrier"):
        pl.semaphore_wait(barrier, n_ep - 1 + ny - 1 + 1)

    disp = {
        d: remote(outgo_ref.at[slot_rows(flip(d))], arrived.at[held(d), lanes_of(tp)],
                  disp_s.at[0], disp_r.at[d - 1], flip(d), tp)
        for d in range(1, n_ep)
    }

    def kv_line(b, target, sem):
        block = kvbuf.at[b * 2 + side]
        return remote(block, block, kz_s.at[sem], kz_r.at[b], target * 2 + side, tp)

    def kv_pass(b):
        block = kvbuf.at[b * 2 + side]
        return remote(block, block, kx_s.at[b], kx_r.at[b], mate, tp)

    has_next = col < nz - 1
    has_prev = col > 0

    for d in groups[0]:
        if d:
            disp[d].start()
    kv_pass(col).start()

    @pl.when(has_next)
    def _():
        kv_line(col, col + 1, col).start()

    @pl.when(has_prev)
    def _():
        kv_line(col, col - 1, nz).start()

    for d in groups[1]:
        disp[d].start()
    ins[12].wait()
    for i in range(starts[0]):
        w_send(i)
    w_partner().start()
    ins[8].wait()
    ins[9].wait()
    q_gain = jnp.concatenate([qg_ref[...], qg_ref[...]], axis=1)
    for g in range(max(1, heads // 2)):
        for b in range(blocks):
            at = slice(b * GRID_W, (b + 1) * GRID_W)
            if heads == 1:
                values = q_in[at, :].astype(f32)
                values = jnp.concatenate([values, jnp.zeros_like(values)], axis=1)
            else:
                values = q_in[at, g * lane_count : (g + 1) * lane_count].astype(f32)
            values = turned(values, q_gain, b) * (head ** (-0.5))
            for h in range(min(2, heads)):
                one = values if h == 0 else pltpu.roll(values, head, 1)
                one = jnp.where(first, one, 0.0).astype(bf16)
                for i in range(max(1, GRID_W // piece)):
                    size = min(piece, GRID_W)
                    token = b * GRID_W + i * size
                    row_at = (token // piece * heads + 2 * g + h) * piece + token % piece
                    q_ref[row_at : row_at + size, :] = one[i * size : (i + 1) * size, :]

    mine_rows = placed_ref[slot_rows(ep), :]
    for q in range(n_tp):
        at = slice(q * dq, (q + 1) * dq)
        full = (x_ref[:, at].astype(f32) * scale * pre_ref[:, at]).astype(bf16)
        arrived[held(0), at] = jnp.dot(mine_rows, full, preferred_element_type=f32).astype(bf16)

    q_rows = q_ref.shape[0]
    tile = min(512, heads * piece)

    def prepare(e, slot):
        keys = kvbuf[e]
        lanes = lax.broadcasted_iota(jnp.int32, keys.shape, 1)
        kt[slot] = keys.T
        vx[slot] = jnp.where(lanes < keys.shape[1] // 2, jnp.ones_like(keys), keys)

    def attend_rows(i, slot, fresh):
        for sub in range(2):
            at = pl.ds(pl.multiple_of(i * 2 * tile + sub * tile, tile), tile)
            scores = jnp.dot(q_ref[at, :], kt[slot], preferred_element_type=f32)
            weights = jnp.exp(scores).astype(bf16)
            term = jnp.dot(weights, vx[slot], preferred_element_type=f32)
            if fresh:
                acc[at, :] = term
            else:
                acc[at, :] += term

    def attend(e, fresh):
        prepare(e, 0)

        for i in range(q_rows // (2 * tile)):
            attend_rows(i, 0, fresh)

    shorter = jnp.minimum(col, nz - 1 - col)
    longer = jnp.where(col <= nz - 1 - col, 1, -1)

    def line_step(k):
        both = k < 2 * shorter
        way = jnp.where(both, 2 * lax.rem(k, 2) - 1, longer)
        far = jnp.where(both, lax.div(k, 2) + 1, k - shorter + 1)
        return col + way * far, col - way

    def line_one(k):
        b, target = line_step(k)
        wait("kv_line", kv_line(b, target, b))

        @pl.when(jnp.logical_and(target >= 0, target <= nz - 1))
        def _():
            kv_line(b, target, b).start()

        kv_pass(b).start()

    def line_take(k):
        both = k < 2 * shorter
        opening = jnp.logical_or(lax.rem(k, 2) == 0, jnp.logical_not(both))

        @pl.when(opening)
        def _():
            line_one(k)

        @pl.when(jnp.logical_and(opening, both))
        def _():
            line_one(k + 1)

    def line_end(early):
        middle = shorter > 0

        @pl.when(middle if early else jnp.logical_not(middle))
        def _():
            line_one(nz - 1 - 1)

    def line_block(k):
        return line_step(k)[0] * 2 + side

    def pass_block(k):
        b, _ = line_step(k)
        wait("kv_pass", kv_pass(b))
        return b * 2 + 1 - side

    def take(k, carry):
        line_take(k)
        attend(line_block(k), False)
        attend(pass_block(k), False)
        return carry

    def relay(d, dy):
        block = arrived.at[held(d), lanes_of(tp)]
        c = 0 if d in groups[0] else 1
        return remote(block, block, rel_s.at[c, dy - 1], rel_r.at[c, dy - 1], ep, same_core(dy))

    def relay_all(c, dy):
        block = arrived.at[foreign(c), lanes_of(row_from(dy) * 2 + core)]
        return remote(block, block, rel_s.at[c, dy - 1], rel_r.at[c, dy - 1], ep, same_core(dy))

    def foreign(c):
        count = len(groups[c]) - (1 if 0 in groups[c] else 0)
        return pl.ds(c * chunk, count * cap)

    def cross(c, dy):
        block = arrived.at[foreign(c), lanes_of(row_from(dy) * 2 + core)]
        if dy == 0:
            return remote(block, block, c0_s.at[c], c0_r.at[c], ep, partner)
        return remote(block, block, cy_s.at[c, dy - 1], cy_r.at[c, dy - 1], ep, partner)

    def relay_chunk(c):
        for d in groups[c]:
            if d:
                wait("disp", disp[d])
                for dy in range(1, ny):
                    relay(d, dy).start()
        cross(c, 0).start()

    def cross_chunk(c):
        for dy in range(1, ny):
            wait("relay", relay_all(c, dy))
            cross(c, dy).start()

    ff = wg_hbm.shape[1]
    step = min(512, ff)

    def m1(c):
        return remote(pm.at[c, 1 - core], pm_in.at[c], m1_s.at[c], m1_r.at[c], ep, partner)

    def m2(c, s, dy):
        at = pl.ds(s * part, part)
        return remote(pm_red.at[c, lax.rem(row + dy, ny), at], pm_in2.at[c, row, at],
                      m2_s.at[c, dy - 1], m2_r.at[c, s, dy - 1], ep, same_core(dy))

    def chunk_rows(c):
        return slice(c * chunk, (c + 1) * chunk)

    def m2_all(c, dy):
        return remote(pm_red.at[c, row], pm_in2.at[c, row], m2_s.at[c, dy - 1], m2_r.at[c, 0, dy - 1], ep, partner)

    def experts_up(c):
        for dy in range(ny):
            wait("cross", cross(c, dy))
        if c == 0:
            loads[0].wait()
            loads[1].wait()
        rows = chunk_rows(c)

        def gated(i, carry):
            at = pl.ds(pl.multiple_of(i * step, step), step)
            x = arrived[rows, : wg_hbm.shape[0]]
            gate = jnp.dot(x, wg[:, at], preferred_element_type=f32)
            up = jnp.dot(x, wu[:, at], preferred_element_type=f32)
            hidden[rows, at] = (gate / (1.0 + jnp.exp(-gate)) * up).astype(bf16)
            return carry

        lax.fori_loop(0, ff // step, gated, 0)

    def experts_down(c):
        rows = chunk_rows(c)
        if c == 0:
            loads[2].wait()

        def down_for(which):
            for y in range(ny):
                cols = pl.ds(pl.multiple_of((y * 2 + which) * dq, dq), dq)
                pm[c, which, y] = jnp.dot(
                    hidden[rows, :ff], wd[:, cols], preferred_element_type=f32
                ).astype(bf16)

        down_for(1 - core)
        m1(c).start()
        down_for(core)

    def reduce_cores(c):
        wait("m1", m1(c))
        for y in range(ny):
            pm_red[c, y] = (pm[c, core, y].astype(f32) + pm_in[c, y].astype(f32)).astype(bf16)
        for s in range(2):
            for dy in range(1, ny):
                m2(c, s, dy).start()

    def back(d):
        return remote(summed.at[held(d)], ret.at[slot_rows(ep)], ret_s.at[0], ret_r.at[0], flip(d), tp)

    def back_all():
        at = pl.ds(0, (n_ep - 1) * cap)
        return remote(summed.at[at], ret.at[at], ret_s.at[0], ret_r.at[0], mate, tp)

    def disp_all():
        at = pl.ds(0, (n_ep - 1) * cap)
        return remote(outgo_ref.at[at], summed.at[at], disp_s.at[0], disp_r.at[0], mate, tp)

    def send_back(c):
        for s in range(2):
            for dy in range(1, ny):
                wait("m2", m2(c, s, dy))
            at = slice(s * part, (s + 1) * part)
            total = pm_red[c, row, at].astype(f32)
            for dy in range(1, ny):
                total = total + pm_in2[c, row_from(dy), at].astype(f32)
            total = total.astype(bf16)
            rows_at = c * chunk + s * part
            summed[rows_at : rows_at + part, :] = total
            for d in order[rows_at // cap : (rows_at + part) // cap]:
                if d:
                    back(d).start()
                else:
                    low = order.index(0) * cap - rows_at
                    ret[slot_rows(ep), :] = total[low : low + cap, :]

    tall = heads * piece
    half = acc.shape[1] // 2

    def finish(target):
        for slot in range(2):
            for i in range(2 * tall // (2 * tile)):
                attend_rows(target * (tall // tile) + i, slot, False)
        sides = []
        for c in range(2):
            which = core if c else 1 - core
            pieces = []
            for h in range(heads):
                at = pl.ds(pl.multiple_of((target * 2 + which) * tall + h * piece, piece), piece)
                sums = acc[at, :]
                pieces.append((sums[:, half:] / sums[:, :half]).astype(bf16))
            sides.append(pieces[0] if heads == 1 else jnp.concatenate(pieces, axis=1))
        return sides

    def a1(d):
        return remote(pa.at[d], pa_in.at[d], a1_s.at[d], a1_r.at[d], ep, partner)

    def a2(d, s):
        at = pl.ds(s * (piece // 2), piece // 2)
        return remote(pa_red.at[d, at], pa_in2.at[d, at], a2_s.at[d - 1], a2_r.at[d - 1, s], ep, same_core(d))

    def a2_all(d):
        return remote(pa_red.at[d], pa_in2.at[d], a2_s.at[d - 1], a2_r.at[d - 1, 0], ep, same_core(d))

    def ho(d, c):
        target = lax.rem(row + d, ny) * 2 + (core if c else 1 - core)
        return remote(ho_out.at[2 * d + c], ho_in.at[tp], ho_s.at[0], ho_r.at[0], ep, target)

    def ho_all():
        block = ho_out.at[pl.ds(0, n_tp - 1)]
        return remote(block, ho_in.at[pl.ds(0, n_tp - 1)], ho_s.at[0], ho_r.at[0], ep, partner)

    def finish_start(d):
        sides = finish(lax.rem(row + d, ny))
        for c in range(2):
            if d == 0 and c == 1:
                ho_in[tp] = sides[1]
            else:
                ho_out[2 * d + c] = sides[c]
                ho(d, c).start()
        both = jnp.concatenate(sides, axis=0)
        total = jnp.dot(both, wout_ref[:, :narrow], preferred_element_type=f32).astype(bf16)
        pa[d] = total[:piece]
        a1(d).start()
        pa_red[d] = total[piece:]

    def finish_end(d):
        wait("a1", a1(d))
        return pa_red[d].astype(f32) + pa_in[d].astype(f32)

    attend(ep, True)
    mixw = mixw_ref[...].T
    high = mixw.astype(bf16)
    mix_high[...] = high
    mix_low[...] = (mixw - high.astype(f32)).astype(bf16)
    relay_chunk(0)
    wait("kv_mate", kv_pass(col))
    attend(mate, False)
    split = max(1, (nz - 1) // 2)
    brief = nz - 2 == split + 1
    line_take(0)
    attend(line_block(0), False)
    relay_chunk(1)
    for i in range(*starts):
        w_send(i)
    cross_chunk(0)
    attend(pass_block(0), False)
    lax.fori_loop(1, split, take, 0)
    if brief:
        line_end(True)
    with jax.named_scope("up0"):
        experts_up(0)
    line_take(split)
    with jax.named_scope("down0"):
        experts_down(0)
    cross_chunk(1)
    attend(line_block(split), False)
    reduce_cores(0)
    for i in range(starts[1], parts):
        w_send(i)
    if brief:
        line_end(False)
    with jax.named_scope("up1"):
        experts_up(1)
    with jax.named_scope("down1"):
        experts_down(1)
    attend(pass_block(split), False)
    lax.fori_loop(split + 1, nz - 2, take, 0)
    if not brief:
        line_take(nz - 2)
    reduce_cores(1)
    prepare(line_block(nz - 2), 0)
    prepare(pass_block(nz - 2), 1)
    ins[10].wait()
    ins[11].wait()
    for d in range(1, ny):
        with jax.named_scope("finish"):
            finish_start(d)
    send_back(0)
    for dy in range(1, ny):
        wait("w_row", w_row_all(dy))
        w_cross(dy).start()
    for d in range(1, ny):
        pa_red[d] = finish_end(d).astype(bf16)
        for s in range(2):
            a2(d, s).start()
    with jax.named_scope("finish"):
        finish_start(0)
    send_back(1)
    pa_red[0] = finish_end(0).astype(bf16)
    wait("w_partner", w_partner())
    for dy in range(1, ny):
        wait("w_cross", w_cross(dy))
    wait("ho", ho_all())
    gathered = jnp.concatenate([ho_in[t] for t in range(n_tp)], axis=1)
    whole[...] = jnp.dot(gathered, wall[:, :wide], preferred_element_type=f32)
    for s in range(2):
        at = slice(s * (piece // 2), (s + 1) * (piece // 2))
        mixed = pa_red[0, at].astype(f32)
        for d in range(1, ny):
            wait("a2", a2(d, s))
            mixed = mixed + pa_in2[d, at].astype(f32)
        rest = whole[at, :]
        square = jnp.sum(mixed * mixed, axis=-1, keepdims=True) + jnp.sum(rest * rest, axis=-1, keepdims=True)
        scale = lax.rsqrt(square * (1.0 / (narrow + wide)) + EPSILON)
        attn_ref[at, :narrow] = (mixed * scale * gain_ref[:, :narrow]).astype(bf16)
        attn_ref[at, narrow:] = (rest * scale * gain_ref[:, narrow:]).astype(bf16)

    wait("back", back_all())
    moe_ref[...] = (
        jnp.dot(mix_high[...], ret[...], preferred_element_type=f32)
        + jnp.dot(mix_low[...], ret[...], preferred_element_type=f32)
    ).astype(bf16)

    sent = [kv_pass(col), disp_all(), back_all(), ho_all(), w_partner()]
    sent += [relay_all(c, dy) for c in range(2) for dy in range(1, ny)]
    sent += [cross(c, dy) for c in range(2) for dy in range(ny)]
    sent += [m1(c) for c in range(2)]
    sent += [m2_all(c, dy) for c in range(2) for dy in range(1, ny)]
    sent += [w_row_all(dy) for dy in range(1, ny)]
    sent += [w_cross(dy) for dy in range(1, ny)]
    sent += [a1(d) for d in range(ny)] + [a2_all(d) for d in range(1, ny)]
    for copy in sent:
        copy.wait_send()

    @pl.when(has_next)
    def _():
        kv_line(col, col + 1, col).wait_send()

    @pl.when(has_prev)
    def _():
        kv_line(col, col - 1, nz).wait_send()

    def kv_done(k, carry):
        b, target = line_step(k)

        @pl.when(jnp.logical_and(target >= 0, target <= nz - 1))
        def _():
            kv_line(b, target, b).wait_send()

        kv_pass(b).wait_send()
        return carry

    lax.fori_loop(0, nz - 1, kv_done, 0)


def hand_over(attn_ref, moe_ref, attn_hbm, moe_hbm, sem):
    copies = [
        pltpu.make_async_copy(attn_ref, attn_hbm, sem.at[0]),
        pltpu.make_async_copy(moe_ref, moe_hbm, sem.at[1]),
    ]
    for copy in copies:
        copy.start()
    for copy in copies:
        copy.wait()


def per_device(
    n_ep, n_tp,
    q_in, k_in, v_in, q_gain, k_gain, w_out, post_gain,
    moe_in, routes, route_logits, pre_gain, w_gate, w_up, w_down,
):
    bf16 = jnp.bfloat16
    head = q_gain.shape[0]
    rows = q_in.shape[0]
    heads = q_in.shape[1] // head
    kv_count = k_in.shape[1] // head
    repeat = heads * n_tp // kv_count
    ny = n_tp // 2
    nz = n_ep // 2
    turns = turn_tables(n_ep * rows, GRID_W, head // 4)

    tokens, top = routes.shape
    width = moe_in.shape[1]
    dq = width // n_tp
    need = max(2, 3 * top * tokens // (2 * n_ep))
    cap = -(-need // 16) * 16
    slots = n_ep * cap

    piece = rows // n_tp
    ff = w_gate.shape[2]
    narrow = width * 4 // 8
    dma = pltpu.SemaphoreType.DMA
    vmem = pl.BlockSpec(memory_space=pltpu.VMEM)
    hbm = pl.BlockSpec(memory_space=pl.ANY)
    outs = pl.pallas_call(
        functools.partial(kernel, (n_ep, n_tp, heads, cap, repeat)),
        out_shape=(
            pltpu.VMEM((piece, width), bf16),
            pltpu.VMEM((tokens, dq), bf16),
        ),
        in_specs=[hbm] * 15,
        out_specs=(vmem, vmem),
        scratch_shapes=[
            pltpu.VMEM((top, tokens), jnp.int32),
            pltpu.VMEM((top, tokens), jnp.float32),
            pltpu.VMEM((1, width), jnp.float32),
            pltpu.VMEM((1, width), jnp.float32),
            pltpu.VMEM((1, head), jnp.float32),
            pltpu.VMEM((1, head), jnp.float32),
            pltpu.VMEM(turns.shape, jnp.float32),
            pltpu.VMEM((rows, heads * head), bf16),
            pltpu.VMEM((rows, 2 * head), bf16),
            pltpu.VMEM((rows, 2 * head), bf16),
            pltpu.VMEM((tokens, width), bf16),
            pltpu.VMEM((heads * head, narrow + SKEW), bf16),
            pltpu.VMEM((heads * rows, 2 * head), bf16),
            pltpu.VMEM((slots, tokens), bf16),
            pltpu.VMEM((slots, dq), bf16),
            pltpu.VMEM((slots, tokens), jnp.float32),
            pltpu.VMEM((width, ff + SKEW), bf16),
            pltpu.VMEM((width, ff + SKEW), bf16),
            pltpu.VMEM((ff, width + SKEW), bf16),
            pltpu.VMEM((n_ep, rows, 2 * head), bf16),
            pltpu.VMEM((2, rows, 2 * head), bf16),
            pltpu.VMEM((2, 2 * head, rows), bf16),
            pltpu.VMEM((heads * rows, 2 * head), jnp.float32),
            pltpu.VMEM((slots, width + SKEW), bf16),
            pltpu.VMEM((slots, ff + SKEW), bf16),
            pltpu.VMEM((tokens, slots), bf16),
            pltpu.VMEM((tokens, slots), bf16),
            pltpu.VMEM((n_tp * heads * head, width - narrow + SKEW), bf16),
            pltpu.VMEM((n_tp, piece, heads * head), bf16),
            pltpu.VMEM((n_tp, piece, heads * head), bf16),
            pltpu.VMEM((piece, width - narrow), jnp.float32),
            pltpu.VMEM((ny, piece, narrow), bf16),
            pltpu.VMEM((ny, piece, narrow), bf16),
            pltpu.VMEM((ny, piece, narrow), bf16),
            pltpu.VMEM((ny, piece, narrow), bf16),
            pltpu.VMEM((2, 2, ny, slots // 2, dq), bf16),
            pltpu.VMEM((2, ny, slots // 2, dq), bf16),
            pltpu.VMEM((2, ny, slots // 2, dq), bf16),
            pltpu.VMEM((2, ny, slots // 2, dq), bf16),
            pltpu.VMEM((slots, dq), bf16),
            pltpu.VMEM((slots, dq), bf16),
            dma((13,)), dma((3,)),
            dma((nz + 1,)), dma((nz,)), dma((nz,)), dma((nz,)),
            dma((1,)), dma((n_ep - 1,)), dma((2, ny - 1)), dma((2, ny - 1)),
            dma((2,)), dma((2,)), dma((2, ny - 1)), dma((2, ny - 1)),
            dma((1,)), dma((1,)), dma((ny - 1,)), dma((ny - 1,)), dma((ny - 1,)), dma((ny - 1,)), dma((1,)), dma((1,)),
            dma((ny,)), dma((ny,)), dma((ny - 1,)), dma((ny - 1, 2)),
            dma((2,)), dma((2,)), dma((2, ny - 1)), dma((2, 2, ny - 1)),
            dma((1,)), dma((1,)),
        ],
        compiler_params=pltpu.CompilerParams(
            collective_id=0, has_side_effects=True, vmem_limit_bytes=VMEM_LIMIT
        ),
    )(
        routes.T, route_logits.T, pre_gain[None, :], post_gain[None, :], q_gain[None, :], k_gain[None, :], turns,
        q_in, k_in, v_in, moe_in, w_out, w_gate[0], w_up[0], w_down[0],
    )
    return pl.pallas_call(
        hand_over,
        out_shape=(
            jax.ShapeDtypeStruct((piece, width), bf16),
            jax.ShapeDtypeStruct((tokens, dq), bf16),
        ),
        in_specs=[vmem, vmem],
        out_specs=(hbm, hbm),
        scratch_shapes=[dma((2,))],
        compiler_params=pltpu.CompilerParams(vmem_limit_bytes=2 * 1024 * 1024),
    )(*outs)


def solution(mesh):
    return jax.shard_map(
        functools.partial(per_device, mesh.shape["ep"], mesh.shape["tp"]),
        mesh=mesh,
        in_specs=(
            P("ep", "tp"),
            P("ep", None),
            P("ep", None),
            P(),
            P(),
            P("tp", None),
            P(),
            P("ep", None),
            P("ep", None),
            P("ep", None),
            P(),
            P("ep", None, "tp"),
            P("ep", None, "tp"),
            P("ep", "tp", None),
        ),
        out_specs=(P(("ep", "tp"), None), P("ep", "tp")),
        check_vma=False,
    )
```
